256 devices in a mesh: ep: 64 (over z, x, core), tp: 4 (over y).
Axes of the slice: x: 4, y: 4, z: 8, core: 2. Of those that a mesh axis runs over, the one named last changes fastest.
Arguments:
- out_gate: bfloat16 [32768, 2048], P(('ep', 'tp')), may hold values from -6 to 6
- in_gate: bfloat16 [32768, 2048], P(('ep', 'tp')), may hold values from -6 to 6
- conv_input: bfloat16 [32768, 2048], P(('ep', 'tp')), may hold values from -6 to 6
- conv_taps: bfloat16 [3, 2048], replicated, may hold values from -3 to 3
- mixer_weight: bfloat16 [2048, 2048], P(None, 'tp'), may hold values from -0.125 to 0.125
- expert_input: bfloat16 [32768, 2048], P(('ep', 'tp')), may hold values from -6 to 6
- norm_gain: float32 [2048], replicated, may hold values from 0.1 to 1.9
- expert_gate: bfloat16 [64, 2048, 1024], P('ep', None, 'tp'), may hold values from -0.125 to 0.125
- expert_up: bfloat16 [64, 2048, 1024], P('ep', None, 'tp'), may hold values from -0.125 to 0.125
- expert_down: bfloat16 [64, 1024, 2048], P('ep', 'tp'), may hold values from -0.1875 to 0.1875
- expert_ids: int32 [32768, 2], P(('ep', 'tp')), may hold values from 0 to 63, all different within a row; in each aligned block of 128 rows (0 to 127, 128 to 255, ...) at most 8 rows name the same one
- route_weight: float32 [32768, 2], P(('ep', 'tp')), may hold values from 0.1 to 1
Outputs:
- mixer_out: bfloat16 [32768, 2048], P('ep', 'tp')
- experts_out: bfloat16 [32768, 2048], P(('ep', 'tp'))
The draws below stay inside these ranges and needn't reach their ends.
Inputs may be any that keep to these rules, and one draw needn't show every extreme that they name: `expert_ids`: each row names 2 different experts. Within the 128 rows of one device no expert is named by more than 8 rows, and in some devices' rows some expert is named by exactly 8.
All inputs are finite; a program needn't handle non-finite values.
Results may differ from the reference program's by a relative error of at most 0.011.
Values may be sent and summed in bfloat16 or wider, within the bound.
No kernel may reach another device: no remote copies, remote signals or barrier semaphores. Data moves between devices by JAX's collectives and lax.ppermute only.
A program may use at most 128 MiB of HBM per device.

```python
import math
import jax
import jax.numpy as jnp
import numpy as np
from jax import lax

D = 2048
FF = 1024
TOP = 2
CONV = 3
SEQS = 1
TOK_DEV = 128
TOKENS = 32768
EXPERTS = 64
CAP = 8
N_TP = 4


def shard_levels(own_key, dims, cuts, smallest, largest):
    level = 1.0
    for dim, shards_of in cuts:
        heights = jax.random.uniform(jax.random.fold_in(jax.random.fold_in(own_key, 6), dim), (shards_of,), jnp.float32, smallest / len(cuts), largest / len(cuts))
        level = level * jnp.repeat(jnp.exp(heights), dims[dim] // shards_of).reshape((-1,) + (1,) * (len(dims) - 1 - dim))
    return level


def deal_out(key, own, number, rows, amount, top, most, slope):
    sequence = jax.random.permutation(key, amount)
    heavy_load, ordinary = load_shares(amount, rows * top, most, slope, True), load_shares(amount, rows * top, most, slope, False)
    places = jnp.arange(amount)

    def named(lengths, offset_by):
        used = int((lengths > 0).sum())
        fixed = max(1, used // 4)
        passed = fixed + (places - fixed + offset_by * (used - fixed)) % max(1, amount - fixed)
        return jnp.zeros((amount,), jnp.int32).at[sequence[jnp.where(places < fixed, places, passed)]].set(jnp.asarray(lengths, jnp.int32))

    lengths = jnp.where(number % 4 == 0, named(heavy_load, number // 4), named(ordinary, number - number // 4 - 1))
    mixed = jax.random.permutation(jax.random.fold_in(own, 3), amount)
    source_of, taker = mixed[0:amount // 2 * 2:2], mixed[1:amount // 2 * 2:2]
    slack = jnp.minimum(lengths[source_of] - 1, most - lengths[taker]) // 2
    slack = jnp.where((source_of == sequence[0]) | (taker == sequence[0]) | (lengths[taker] == 0), 0, jnp.maximum(slack, 0))
    passed = jax.random.randint(jax.random.fold_in(own, 4), (amount // 2,), 0, 1 << 20) % (slack + 1)
    lengths = lengths.at[source_of].add(-passed).at[taker].add(passed)
    members = jnp.searchsorted(jnp.cumsum(lengths), jnp.arange(rows * top), side="right").astype(jnp.int32)
    grid = members.reshape(top, rows).T
    grid = grid[jax.random.permutation(jax.random.fold_in(own, 1), rows)]
    offset_by = jax.random.randint(jax.random.fold_in(own, 2), (rows, 1), 0, top)
    return jnp.take_along_axis(grid, (jnp.arange(top)[None, :] + offset_by) % top, axis=1)


def load_shares(number_of, total, most, skew, full):
    loads = [(1 << 20) // math.isqrt(standing ** skew) + 1 for standing in range(1, number_of + 1)]
    largest = most if full else min(most, max(-(-total // number_of), total * loads[0] // sum(loads)))
    least = 1 if total - largest >= number_of - 1 else 0
    given, surplus = [largest] + [least] * (number_of - 1), total - largest - least * (number_of - 1)
    while surplus > 0:
        free = [i for i in range(1, number_of) if given[i] < largest] or [i for i in range(1, number_of) if given[i] < most]
        mass, left = sum([loads[i] for i in free]), surplus
        for i in free:
            addition = min(most - given[i], max(1, left * loads[i] // mass), surplus)
            given[i] = given[i] + addition
            surplus = surplus - addition
    return np.array(given)


def normal_values(key, extent, spread, most, pieces=(), held_as=jnp.bfloat16):
    array = spread * jax.random.normal(key, extent, jnp.float32)
    if pieces:
        array = array * shard_levels(key, extent, pieces, -0.22, 0.18)
    return jnp.clip(array, -most, most).astype(held_as)


def setup_inputs(seed: int = 0) -> dict:
    seeds = jax.random.split(jax.random.key(seed), 13)
    out_gate = normal_values(seeds[0], (TOKENS, D), 1.0, 6.0, ((0, 256),))
    in_gate = normal_values(seeds[1], (TOKENS, D), 1.0, 6.0, ((0, 256),))
    conv_input = normal_values(seeds[2], (TOKENS, D), 1.0, 6.0, ((0, 256),))
    conv_taps = normal_values(seeds[3], (CONV, D), 0.577, 3.0)
    mixer_weight = normal_values(seeds[4], (D, D), D ** -0.5, 0.125, ((1, 4),))
    expert_input = normal_values(seeds[5], (TOKENS, D), 1.0, 6.0, ((0, 256),))
    norm_gain = jnp.clip(1.0 + 0.18 * jax.random.normal(seeds[6], (D,), jnp.float32), 0.1, 1.9)
    expert_gate = normal_values(seeds[7], (EXPERTS, D, FF), D ** -0.5, 0.125, ((0, 64), (2, 4)))
    expert_up = normal_values(seeds[8], (EXPERTS, D, FF), D ** -0.5, 0.125, ((0, 64), (2, 4)))
    expert_down = normal_values(seeds[9], (EXPERTS, FF, D), FF ** -0.5, 0.1875, ((0, 64), (1, 4)))
    expert_ids_keys = jax.random.split(jax.random.fold_in(seeds[10], 1), TOKENS // TOK_DEV)
    expert_ids_turns = jax.random.permutation(jax.random.fold_in(seeds[10], 3), TOKENS // TOK_DEV)
    expert_ids = jax.vmap(lambda own, number: deal_out(jax.random.fold_in(seeds[10], 2), own, number, TOK_DEV, EXPERTS, TOP, CAP, 1))(expert_ids_keys, expert_ids_turns).reshape((TOKENS, TOP))
    route_weight = jnp.clip(jnp.exp(math.log(1.0) - 2.3025851 * jax.random.uniform(seeds[11], (TOKENS, TOP), jnp.float32) ** shard_levels(seeds[11], (TOKENS, TOP), ((0, 256),), -0.2, 0.2)), 0.1, 1.0)
    return {"out_gate": out_gate, "in_gate": in_gate, "conv_input": conv_input, "conv_taps": conv_taps, "mixer_weight": mixer_weight, "expert_input": expert_input, "norm_gain": norm_gain, "expert_gate": expert_gate, "expert_up": expert_up, "expert_down": expert_down, "expert_ids": expert_ids, "route_weight": route_weight}


norm_eps = 1e-06

def device_slots(route_ids, expert_count):
    flat_ids = route_ids.reshape(-1)
    member = (flat_ids[:, None] == jnp.arange(expert_count, dtype=jnp.int32)[None, :]).astype(jnp.int32)
    before = jnp.cumsum(member, axis=0) - member
    return lax.optimization_barrier(jnp.sum(before * member, axis=1)).astype(jnp.int32).reshape(route_ids.shape)

def short_conv(out_gate, in_gate, conv_input, conv_taps, mixer_weight):
    product = in_gate.astype(jnp.float32) * conv_input.astype(jnp.float32)
    seq_length = TOKENS // SEQS
    by_sequence = product.reshape(SEQS, seq_length, D)
    padded = jnp.pad(by_sequence, ((0, 0), (CONV - 1, 0), (0, 0)))
    tap_values = conv_taps.astype(jnp.float32)
    smoothed = sum((padded[:, tap_index:tap_index + seq_length] * tap_values[tap_index] for tap_index in range(CONV)))
    gated = (out_gate.astype(jnp.float32) * smoothed.reshape(TOKENS, D)).astype(jnp.bfloat16)
    return jnp.dot(gated, mixer_weight, preferred_element_type=jnp.float32).astype(jnp.bfloat16)

def routed_experts(expert_input, norm_gain, expert_gate, expert_up, expert_down, expert_ids, route_weight):
    wide_input = expert_input.astype(jnp.float32)
    inv_norm = lax.rsqrt(lax.optimization_barrier(jnp.mean(wide_input * wide_input, axis=1, keepdims=True)) + norm_eps)
    normed = (wide_input * inv_norm * norm_gain.astype(jnp.float32)).astype(jnp.bfloat16)
    devices = TOKENS // TOK_DEV
    block_ids = expert_ids.reshape(devices, TOK_DEV, TOP).astype(jnp.int32)

    def block_slots(route_ids):
        return device_slots(route_ids, EXPERTS)
    slot_rank = jax.vmap(block_slots)(block_ids)
    device_index = jnp.arange(devices, dtype=jnp.int32)[:, None, None]
    slot_index = (device_index * CAP + slot_rank).astype(jnp.int32)
    token_index = (device_index * TOK_DEV + jnp.arange(TOK_DEV, dtype=jnp.int32)[None, :, None] + jnp.zeros_like(slot_rank)).astype(jnp.int32)
    slot_table = jnp.zeros((EXPERTS, devices * CAP), jnp.int32).at[block_ids, slot_index].set(token_index)
    fourth = FF // N_TP

    def one_expert(operands):
        token_rows, w_gate, w_up, w_down = operands
        slot_rows = normed[token_rows]
        gate_proj = jnp.dot(slot_rows, w_gate, preferred_element_type=jnp.float32)
        up_proj = jnp.dot(slot_rows, w_up, preferred_element_type=jnp.float32)
        hidden = (jax.nn.silu(gate_proj) * up_proj).astype(jnp.bfloat16)
        running = jnp.zeros((slot_rows.shape[0], D), jnp.float32)
        for quarter in range(N_TP):
            partial_sum = jnp.dot(hidden[:, quarter * fourth:(quarter + 1) * fourth], w_down[quarter * fourth:(quarter + 1) * fourth], preferred_element_type=jnp.float32)
            running = running + lax.optimization_barrier(partial_sum.astype(jnp.bfloat16)).astype(jnp.float32)
        return running.astype(jnp.bfloat16)
    results = lax.map(one_expert, (slot_table, expert_gate, expert_up, expert_down))
    picked = results[block_ids, slot_index].reshape(TOKENS, TOP, D).astype(jnp.float32)
    route_share = route_weight / lax.optimization_barrier(jnp.sum(route_weight, axis=1, keepdims=True))
    return lax.optimization_barrier(jnp.sum(picked * route_share[:, :, None], axis=1)).astype(jnp.bfloat16)

def reference(out_gate, in_gate, conv_input, conv_taps, mixer_weight, expert_input, norm_gain, expert_gate, expert_up, expert_down, expert_ids, route_weight):
    mixer_out = short_conv(out_gate, in_gate, conv_input, conv_taps, mixer_weight)
    experts_out = routed_experts(expert_input, norm_gain, expert_gate, expert_up, expert_down, expert_ids, route_weight)
    return (mixer_out, experts_out)
```

```python
import jax
import jax.numpy as jnp
from jax import lax
from jax.experimental import pallas as pl
from jax.experimental.pallas import tpu as pltpu
from jax.sharding import PartitionSpec as P

CONV = 3
NORM_EPS = 1e-06
FIRST_COLS = 512


def turn(value, steps):
    count = lax.axis_size("tp")
    pairs = [(source, (source + steps) % count) for source in range(count)]
    return lax.ppermute(value, "tp", pairs)


def from_sides(value):
    return turn(value, 1), turn(value, -1)


def from_opposite(left, right):
    half = left.shape[0] // 2
    return turn(left[:half], 1), turn(right[half:], -1)


def slot_table(ids, expert_count, slot_cap):
    tokens = ids.shape[1]
    expert = lax.broadcasted_iota(jnp.int32, (expert_count, tokens), 0)
    chosen = [ids[k : k + 1] == expert for k in range(ids.shape[0])]
    member = jnp.where(chosen[0] | chosen[1], 1.0, 0.0).astype(jnp.bfloat16)
    row = lax.broadcasted_iota(jnp.int32, (tokens, tokens), 0)
    column = lax.broadcasted_iota(jnp.int32, (tokens, tokens), 1)
    earlier = jnp.where(row < column, 1.0, 0.0).astype(jnp.bfloat16)
    before = jnp.dot(member, earlier, preferred_element_type=jnp.float32).astype(jnp.int32)
    shape = (expert_count, slot_cap, tokens)
    slot = lax.broadcasted_iota(jnp.int32, shape, 1)
    here = jnp.broadcast_to(before[:, None, :], shape) == slot
    return [
        jnp.where(here, jnp.broadcast_to(jnp.where(c, 1.0, 0.0)[:, None, :], shape), 0.0).reshape(
            expert_count * slot_cap, tokens
        )
        for c in chosen
    ]


def dispatch_kernel(ids_ref, input_ref, gain_ref, out_ref, *, expert_count, slot_cap):
    wide = input_ref[...].astype(jnp.float32)
    inv_norm = lax.rsqrt(jnp.mean(wide * wide, axis=1, keepdims=True) + NORM_EPS)
    normed = (wide * inv_norm * gain_ref[...]).astype(jnp.bfloat16)
    table = sum(slot_table(ids_ref[...], expert_count, slot_cap)).astype(jnp.bfloat16)
    out_ref[...] = jnp.dot(table, normed, preferred_element_type=jnp.float32).astype(jnp.bfloat16)


def combine_kernel(ids_ref, weight_ref, *refs, expert_count, slot_cap):
    out_ref = refs[-1]
    weight = weight_ref[...]
    share = weight / (weight[0:1] + weight[1:2])
    tables = slot_table(ids_ref[...], expert_count, slot_cap)
    mix = tables[0] * share[0:1] + tables[1] * share[1:2]
    high = mix.astype(jnp.bfloat16)
    low = (mix - high.astype(jnp.float32)).astype(jnp.bfloat16)
    at = 0
    for ref in refs[:-1]:
        rows = ref[...]
        picked = sum(
            lax.dot_general(m, rows, (((0,), (0,)), ((), ())), preferred_element_type=jnp.float32)
            for m in (high, low)
        )
        out_ref[:, at : at + rows.shape[1]] = picked.astype(jnp.bfloat16)
        at += rows.shape[1]


def mixer_kernel(place_ref, own_ref, left_ref, right_ref, first_ref, second_ref, weight_ref, out_ref):
    rows = own_ref.shape[0]
    weight = weight_ref[...]

    def put(ref, steps, offset):
        block = jnp.dot(ref[...], weight, preferred_element_type=jnp.float32).astype(jnp.bfloat16)
        at = ((place_ref[0] + steps) & 3) * rows + offset
        out_ref[pl.ds(pl.multiple_of(at, rows // 2), block.shape[0]), :] = block

    put(own_ref, 0, 0)
    put(left_ref, 3, 0)
    put(right_ref, 1, 0)
    put(first_ref, 2, 0)
    put(second_ref, 2, rows // 2)


def dot32(a, b):
    return jnp.dot(a, b, preferred_element_type=jnp.float32)


def local(
    out_gate,
    in_gate,
    conv_input,
    conv_taps,
    mixer_weight,
    expert_input,
    norm_gain,
    expert_gate,
    expert_up,
    expert_down,
    expert_ids,
    route_weight,
):
    row_count, model_width = in_gate.shape
    token_count = expert_input.shape[0]
    expert_count = lax.axis_size("ep")
    slot_cap = 4 * token_count // expert_count
    slots = expert_count * slot_cap
    vmem = pl.BlockSpec(memory_space=pltpu.VMEM)
    ids_t = expert_ids.T
    weight_t = route_weight.T

    gate, up, down = expert_gate[0], expert_up[0], expert_down[0]
    down_parts = (down[:, :FIRST_COLS], down[:, FIRST_COLS:])
    gates = from_sides(gate)
    ups = from_sides(up)
    gates_far = from_opposite(*gates)
    ups_far = from_opposite(*ups)
    downs = []
    for part in down_parts:
        sides = from_sides(part)
        downs.append((part, *sides, *from_opposite(*sides)))

    outgoing = pl.pallas_call(
        lambda *refs: dispatch_kernel(*refs, expert_count=expert_count, slot_cap=slot_cap),
        out_shape=jax.ShapeDtypeStruct((slots, model_width), jnp.bfloat16),
        in_specs=[vmem] * 3,
        out_specs=vmem,
        name="dispatch",
    )(ids_t, expert_input, norm_gain[None])
    arrived = lax.all_to_all(
        outgoing.reshape(expert_count, slot_cap, model_width), "ep", 0, 0, tiled=True
    ).reshape(slots, model_width)

    tap_span = CONV - 1
    product = in_gate.astype(jnp.float32) * conv_input.astype(jnp.float32)
    devices = expert_count * lax.axis_size("tp")
    earlier = lax.ppermute(
        product[row_count - tap_span :], ("ep", "tp"), [(i, i + 1) for i in range(devices - 1)]
    )
    padded = jnp.concatenate([earlier, product], axis=0)
    taps = conv_taps.astype(jnp.float32)
    smoothed = sum(padded[j : j + row_count] * taps[j] for j in range(CONV))
    gated = (out_gate.astype(jnp.float32) * smoothed).astype(jnp.bfloat16)

    half = model_width // 2
    hidden = []
    for g, u in ((gate, up), (gates[0], ups[0]), (gates[1], ups[1])):
        hidden.append((jax.nn.silu(dot32(arrived, g)) * dot32(arrived, u)).astype(jnp.bfloat16))
    g = dot32(arrived[:, :half], gates_far[0]) + dot32(arrived[:, half:], gates_far[1])
    u = dot32(arrived[:, :half], ups_far[0]) + dot32(arrived[:, half:], ups_far[1])
    far = (jax.nn.silu(g) * u).astype(jnp.bfloat16)
    middle = far.shape[1] // 2
    hidden += [far[:, :middle], far[:, middle:]]

    returned = []
    for parts in downs:
        result = sum(dot32(h, d) for h, d in zip(hidden, parts)).astype(jnp.bfloat16)
        back = lax.all_to_all(
            result.reshape(expert_count, slot_cap, -1), "ep", 0, 0, tiled=True
        )
        returned.append(back.reshape(slots, -1))

    gated_sides = from_sides(gated)
    gated_far = from_opposite(*gated_sides)
    mixer_out = pl.pallas_call(
        mixer_kernel,
        out_shape=jax.ShapeDtypeStruct((4 * row_count, mixer_weight.shape[1]), jnp.bfloat16),
        in_specs=[pl.BlockSpec(memory_space=pltpu.SMEM)] + [vmem] * 6,
        out_specs=vmem,
        name="mixer",
    )(lax.axis_index("tp").reshape(1), gated, *gated_sides, *gated_far, mixer_weight)

    experts_out = pl.pallas_call(
        lambda *refs: combine_kernel(*refs, expert_count=expert_count, slot_cap=slot_cap),
        out_shape=jax.ShapeDtypeStruct((token_count, model_width), jnp.bfloat16),
        in_specs=[vmem] * 4,
        out_specs=vmem,
        name="combine",
    )(ids_t, weight_t, *returned)
    return (mixer_out, experts_out)


def solution(mesh):
    return jax.shard_map(
        local,
        mesh=mesh,
        in_specs=(
            P(("ep", "tp"), None),
            P(("ep", "tp"), None),
            P(("ep", "tp"), None),
            P(),
            P(None, "tp"),
            P(("ep", "tp"), None),
            P(),
            P("ep", None, "tp"),
            P("ep", None, "tp"),
            P("ep", "tp", None),
            P(("ep", "tp"), None),
            P(("ep", "tp"), None),
        ),
        out_specs=(P("ep", "tp"), P(("ep", "tp"), None)),
        check_vma=False,
    )
```

```python
import jax
import jax.numpy as jnp
from jax import lax
from jax.experimental import pallas as pl
from jax.experimental.pallas import tpu as pltpu
from jax.sharding import PartitionSpec as P


CONV = 3
NORM_EPS = 1e-06
PIECES = (256, 256, 1024, 512)
CHUNKS = ((0, 1), (2, 3))


def turn(value, steps):
    count = lax.axis_size("tp")
    pairs = [(source, (source + steps) % count) for source in range(count)]
    return lax.ppermute(value, "tp", pairs)


def from_sides(value):
    return turn(value, 1), turn(value, -1)


def from_opposite(left, right):
    half = left.shape[0] // 2
    return turn(left[:half], 1), turn(right[half:], -1)


def slot_table(ids, expert_count, slot_cap):
    tokens = ids.shape[1]
    expert = lax.broadcasted_iota(jnp.int32, (expert_count, tokens), 0)
    chosen = [ids[k : k + 1] == expert for k in range(ids.shape[0])]
    member = jnp.where(chosen[0] | chosen[1], 1.0, 0.0).astype(jnp.bfloat16)
    row = lax.broadcasted_iota(jnp.int32, (tokens, tokens), 0)
    column = lax.broadcasted_iota(jnp.int32, (tokens, tokens), 1)
    earlier = jnp.where(row < column, 1.0, 0.0).astype(jnp.bfloat16)
    before = jnp.dot(member, earlier, preferred_element_type=jnp.float32).astype(jnp.int32)
    shape = (expert_count, slot_cap, tokens)
    slot = lax.broadcasted_iota(jnp.int32, shape, 1)
    here = jnp.broadcast_to(before[:, None, :], shape) == slot
    return [
        jnp.where(here, jnp.broadcast_to(jnp.where(c, 1.0, 0.0)[:, None, :], shape), 0.0).reshape(
            expert_count * slot_cap, tokens
        )
        for c in chosen
    ]


def dispatch_kernel(ids_ref, input_ref, gain_ref, out_ref, *, expert_count, slot_cap):
    wide = input_ref[...].astype(jnp.float32)
    inv_norm = lax.rsqrt(jnp.mean(wide * wide, axis=1, keepdims=True) + NORM_EPS)
    normed = (wide * inv_norm * gain_ref[...]).astype(jnp.bfloat16)
    table = sum(slot_table(ids_ref[...], expert_count, slot_cap)).astype(jnp.bfloat16)
    out_ref[...] = jnp.dot(table, normed, preferred_element_type=jnp.float32).astype(jnp.bfloat16)


def mix_kernel(ids_ref, weight_ref, high_ref, low_ref, *, expert_count, slot_cap):
    weight = weight_ref[...]
    share = weight / (weight[0:1] + weight[1:2])
    tables = slot_table(ids_ref[...], expert_count, slot_cap)
    mix = (tables[0] * share[0:1] + tables[1] * share[1:2]).T
    high = mix.astype(jnp.bfloat16)
    high_ref[...] = high
    low_ref[...] = (mix - high.astype(jnp.float32)).astype(jnp.bfloat16)


def combine_kernel(high_ref, low_ref, *refs):
    out_ref, at = refs[-1], 0
    for ref in refs[:-1]:
        rows = ref[...]
        picked = dot32(high_ref[...], rows) + dot32(low_ref[...], rows)
        out_ref[:, at : at + rows.shape[1]] = picked.astype(jnp.bfloat16)
        at += rows.shape[1]


def down_kernel(*refs):
    out_ref, hidden, downs, at = refs[-1], refs[:4], refs[4:-1], 0
    for i in range(0, len(downs), 4):
        own = downs[i]
        total = sum(dot32(h[...], d[...]) for h, d in zip(hidden, downs[i : i + 4]))
        out_ref[:, at : at + own.shape[1]] = total.astype(jnp.bfloat16)
        at += own.shape[1]


def mixer_kernel(place_ref, own_ref, left_ref, right_ref, first_ref, second_ref, weight_ref, out_ref):
    rows = own_ref.shape[0]
    weight = weight_ref[...]

    def put(ref, steps, offset):
        block = jnp.dot(ref[...], weight, preferred_element_type=jnp.float32).astype(jnp.bfloat16)
        at = ((place_ref[0] + steps) & 3) * rows + offset
        out_ref[pl.ds(pl.multiple_of(at, rows // 2), block.shape[0]), :] = block

    put(own_ref, 0, 0)
    put(left_ref, 3, 0)
    put(right_ref, 1, 0)
    put(first_ref, 2, 0)
    put(second_ref, 2, rows // 2)


def dot32(a, b):
    return jnp.dot(a, b, preferred_element_type=jnp.float32)


def local(
    out_gate,
    in_gate,
    conv_input,
    conv_taps,
    mixer_weight,
    expert_input,
    norm_gain,
    expert_gate,
    expert_up,
    expert_down,
    expert_ids,
    route_weight,
):
    row_count, model_width = in_gate.shape
    token_count = expert_input.shape[0]
    expert_count = lax.axis_size("ep")
    slot_cap = 4 * token_count // expert_count
    slots = expert_count * slot_cap
    vmem = pl.BlockSpec(memory_space=pltpu.VMEM)
    ids_t = expert_ids.T
    weight_t = route_weight.T

    gate, up, down = expert_gate[0], expert_up[0], expert_down[0]
    gates = from_sides(gate)
    ups = from_sides(up)
    gate_far = turn(gates[0], 1)
    up_far = turn(ups[1], -1)
    downs, at = [], 0
    for i, width in enumerate(PIECES):
        part = down[:, at : at + width]
        at += width
        sides = from_sides(part)
        far = turn(sides[i % 2], 1 - 2 * (i % 2))
        downs.append((part, *sides, far))

    outgoing = pl.pallas_call(
        lambda *refs: dispatch_kernel(*refs, expert_count=expert_count, slot_cap=slot_cap),
        out_shape=jax.ShapeDtypeStruct((slots, model_width), jnp.bfloat16),
        in_specs=[vmem] * 3,
        out_specs=vmem,
        name="dispatch",
    )(ids_t, expert_input, norm_gain[None])
    arrived = lax.all_to_all(
        outgoing.reshape(expert_count, slot_cap, model_width), "ep", 0, 0, tiled=True
    ).reshape(slots, model_width)
    mix = pl.pallas_call(
        lambda *refs: mix_kernel(*refs, expert_count=expert_count, slot_cap=slot_cap),
        out_shape=[jax.ShapeDtypeStruct((token_count, slots), jnp.bfloat16)] * 2,
        in_specs=[vmem] * 2,
        out_specs=[vmem] * 2,
        name="mix",
    )(ids_t, weight_t)

    tap_span = CONV - 1
    product = in_gate.astype(jnp.float32) * conv_input.astype(jnp.float32)
    devices = expert_count * lax.axis_size("tp")
    earlier = lax.ppermute(
        product[row_count - tap_span :], ("ep", "tp"), [(i, i + 1) for i in range(devices - 1)]
    )
    padded = jnp.concatenate([earlier, product], axis=0)
    taps = conv_taps.astype(jnp.float32)
    smoothed = sum(padded[j : j + row_count] * taps[j] for j in range(CONV))
    gated = (out_gate.astype(jnp.float32) * smoothed).astype(jnp.bfloat16)

    hidden = [
        (jax.nn.silu(dot32(arrived, g)) * dot32(arrived, u)).astype(jnp.bfloat16)
        for g, u in zip((gate, *gates, gate_far), (up, *ups, up_far))
    ]

    returned = []
    for chunk in CHUNKS:
        operands = [d for piece in chunk for d in downs[piece]]
        width = sum(PIECES[piece] for piece in chunk)
        result = pl.pallas_call(
            down_kernel,
            out_shape=jax.ShapeDtypeStruct((slots, width), jnp.bfloat16),
            in_specs=[vmem] * (4 + len(operands)),
            out_specs=vmem,
        )(*hidden, *operands)
        back = lax.all_to_all(result.reshape(expert_count, slot_cap, width), "ep", 0, 0, tiled=True)
        returned.append(back.reshape(slots, width))

    gated_sides = from_sides(gated)
    gated_far = from_opposite(*gated_sides)
    mixer_out = pl.pallas_call(
        mixer_kernel,
        out_shape=jax.ShapeDtypeStruct((4 * row_count, mixer_weight.shape[1]), jnp.bfloat16),
        in_specs=[pl.BlockSpec(memory_space=pltpu.SMEM)] + [vmem] * 6,
        out_specs=vmem,
        name="mixer",
    )(lax.axis_index("tp").reshape(1), gated, *gated_sides, *gated_far, mixer_weight)

    experts_out = pl.pallas_call(
        combine_kernel,
        out_shape=jax.ShapeDtypeStruct((token_count, model_width), jnp.bfloat16),
        in_specs=[vmem] * (2 + len(returned)),
        out_specs=vmem,
        name="combine",
    )(*mix, *returned)
    return (mixer_out, experts_out)


def solution(mesh):
    return jax.shard_map(
        local,
        mesh=mesh,
        in_specs=(
            P(("ep", "tp"), None),
            P(("ep", "tp"), None),
            P(("ep", "tp"), None),
            P(),
            P(None, "tp"),
            P(("ep", "tp"), None),
            P(),
            P("ep", None, "tp"),
            P("ep", None, "tp"),
            P("ep", "tp", None),
            P(("ep", "tp"), None),
            P(("ep", "tp"), None),
        ),
        out_specs=(P("ep", "tp"), P(("ep", "tp"), None)),
        check_vma=False,
    )
```

```python
import jax
import jax.numpy as jnp
from jax import lax
from jax.experimental import pallas as pl
from jax.experimental.pallas import tpu as pltpu
from jax.sharding import PartitionSpec as P


CONV = 3
NORM_EPS = 1e-06
PIECES = (384, 384, 768, 512)
CHUNKS = (((0, 1), 384), ((2, 3), 256))
DEPTH = 512
COLUMNS = 256


def turn(value, steps):
    count = lax.axis_size("tp")
    pairs = [(source, (source + steps) % count) for source in range(count)]
    return lax.ppermute(value, "tp", pairs)


def from_sides(value):
    return turn(value, 1), turn(value, -1)


def from_opposite(left, right):
    half = left.shape[0] // 2
    return turn(left[:half], 1), turn(right[half:], -1)


def slot_table(ids, expert_count, slot_cap):
    tokens = ids.shape[1]
    expert = lax.broadcasted_iota(jnp.int32, (expert_count, tokens), 0)
    chosen = [ids[k : k + 1] == expert for k in range(ids.shape[0])]
    member = jnp.where(chosen[0] | chosen[1], 1.0, 0.0).astype(jnp.bfloat16)
    row = lax.broadcasted_iota(jnp.int32, (tokens, tokens), 0)
    column = lax.broadcasted_iota(jnp.int32, (tokens, tokens), 1)
    earlier = jnp.where(row < column, 1.0, 0.0).astype(jnp.bfloat16)
    before = jnp.dot(member, earlier, preferred_element_type=jnp.float32).astype(jnp.int32)
    shape = (expert_count, slot_cap, tokens)
    slot = lax.broadcasted_iota(jnp.int32, shape, 1)
    here = jnp.broadcast_to(before[:, None, :], shape) == slot
    return [
        jnp.where(here, jnp.broadcast_to(jnp.where(c, 1.0, 0.0)[:, None, :], shape), 0.0).reshape(
            expert_count * slot_cap, tokens
        )
        for c in chosen
    ]


def dispatch_kernel(ids_ref, input_ref, gain_ref, out_ref, *, expert_count, slot_cap):
    wide = input_ref[...].astype(jnp.float32)
    inv_norm = lax.rsqrt(jnp.mean(wide * wide, axis=1, keepdims=True) + NORM_EPS)
    normed = (wide * inv_norm * gain_ref[...]).astype(jnp.bfloat16)
    table = sum(slot_table(ids_ref[...], expert_count, slot_cap)).astype(jnp.bfloat16)
    out_ref[...] = jnp.dot(table, normed, preferred_element_type=jnp.float32).astype(jnp.bfloat16)


def mix_kernel(ids_ref, weight_ref, out_ref, *, expert_count, slot_cap):
    weight = weight_ref[...]
    tokens = weight.shape[1]
    share = weight / (weight[0:1] + weight[1:2])
    tables = slot_table(ids_ref[...], expert_count, slot_cap)
    mix = (tables[0] * share[0:1] + tables[1] * share[1:2]).T
    high = mix.astype(jnp.bfloat16)
    out_ref[:tokens] = high
    out_ref[tokens:] = (mix - high.astype(jnp.float32)).astype(jnp.bfloat16)


def combine_kernel(mix_ref, rows_ref, *refs):
    out_ref = refs[-1]
    both = dot32(mix_ref[...], rows_ref[...])
    tokens = out_ref.shape[0]
    out_ref[...] = (both[:tokens] + both[tokens:]).astype(jnp.bfloat16)


def combine(mix, rows, at, width, before):
    tokens, slots = mix.shape[0] // 2, mix.shape[1]
    first = at // COLUMNS
    return pl.pallas_call(
        combine_kernel,
        out_shape=jax.ShapeDtypeStruct((tokens, width), jnp.bfloat16),
        grid=(rows.shape[1] // COLUMNS,),
        in_specs=[
            pl.BlockSpec(mix.shape, lambda j: (0, 0)),
            pl.BlockSpec((slots, COLUMNS), lambda j: (0, j)),
        ]
        + [pl.BlockSpec(memory_space=pl.ANY)] * len(before),
        out_specs=pl.BlockSpec((tokens, COLUMNS), lambda j: (0, j + first)),
        input_output_aliases={2: 0} if before else {},
    )(mix, rows, *before)


def hidden_kernel(*refs, count):
    rows = refs[0][...]
    weights, outs, sums = refs[1 : 1 + 2 * count], refs[1 + 2 * count : 1 + 3 * count], refs[1 + 3 * count :]
    step = pl.program_id(0)
    products = [dot32(rows, w[...]) for w in weights]

    @pl.when(step == 0)
    def _():
        for total, product in zip(sums, products):
            total[...] = product

    @pl.when(step > 0)
    def _():
        for total, product in zip(sums, products):
            total[...] += product

    @pl.when(step == pl.num_programs(0) - 1)
    def _():
        for i, out in enumerate(outs):
            gate = sums[2 * i][...]
            out[...] = (gate / (1.0 + jnp.exp(-gate)) * sums[2 * i + 1][...]).astype(jnp.bfloat16)


def hidden_of(rows, pairs):
    slots, width = rows.shape
    units = pairs[0][0].shape[1]
    weights = [w for pair in pairs for w in pair]
    return pl.pallas_call(
        lambda *refs: hidden_kernel(*refs, count=len(pairs)),
        out_shape=[jax.ShapeDtypeStruct((slots, units), jnp.bfloat16)] * len(pairs),
        grid=(width // DEPTH,),
        in_specs=[pl.BlockSpec((slots, DEPTH), lambda k: (0, k))]
        + [pl.BlockSpec((DEPTH, units), lambda k: (k, 0))] * len(weights),
        out_specs=[pl.BlockSpec((slots, units), lambda k: (0, 0))] * len(pairs),
        scratch_shapes=[pltpu.VMEM((slots, units), jnp.float32)] * len(weights),
    )(rows, *weights)


def down_kernel(*refs, counts):
    hidden, downs, out_ref = refs[:4], refs[4:-1], refs[-1]
    step, first = pl.program_id(0), 0
    for i, count in enumerate(counts):

        @pl.when((step >= first) & (step < first + count))
        def _():
            total = sum(dot32(h[...], d[...]) for h, d in zip(hidden, downs[4 * i : 4 * i + 4]))
            out_ref[...] = total.astype(jnp.bfloat16)

        first += count


def down_of(hidden, pieces, block):
    slots, units = hidden[0].shape
    counts = [piece[0].shape[1] // block for piece in pieces]
    specs, first = [pl.BlockSpec((slots, units), lambda j: (0, 0))] * 4, 0
    for count in counts:
        specs += [
            pl.BlockSpec(
                (units, block), lambda j, first=first, count=count: (0, jnp.clip(j - first, 0, count - 1))
            )
        ] * 4
        first += count
    return pl.pallas_call(
        lambda *refs: down_kernel(*refs, counts=counts),
        out_shape=jax.ShapeDtypeStruct((slots, first * block), jnp.bfloat16),
        grid=(first,),
        in_specs=specs,
        out_specs=pl.BlockSpec((slots, block), lambda j: (0, j)),
    )(*hidden, *[d for piece in pieces for d in piece])


def mixer_kernel(place_ref, own_ref, left_ref, right_ref, first_ref, second_ref, weight_ref, out_ref):
    rows = own_ref.shape[0]
    weight = weight_ref[...]

    def put(ref, steps, offset):
        block = jnp.dot(ref[...], weight, preferred_element_type=jnp.float32).astype(jnp.bfloat16)
        at = ((place_ref[0] + steps) & 3) * rows + offset
        out_ref[pl.ds(pl.multiple_of(at, rows // 2), block.shape[0]), :] = block

    put(own_ref, 0, 0)
    put(left_ref, 3, 0)
    put(right_ref, 1, 0)
    put(first_ref, 2, 0)
    put(second_ref, 2, rows // 2)


def dot32(a, b):
    return jnp.dot(a, b, preferred_element_type=jnp.float32)


def local(
    out_gate,
    in_gate,
    conv_input,
    conv_taps,
    mixer_weight,
    expert_input,
    norm_gain,
    expert_gate,
    expert_up,
    expert_down,
    expert_ids,
    route_weight,
):
    row_count, model_width = in_gate.shape
    token_count = expert_input.shape[0]
    expert_count = lax.axis_size("ep")
    slot_cap = 4 * token_count // expert_count
    slots = expert_count * slot_cap
    vmem = pl.BlockSpec(memory_space=pltpu.VMEM)
    ids_t = expert_ids.T
    weight_t = route_weight.T

    gate, up, down = expert_gate[0], expert_up[0], expert_down[0]
    gates = from_sides(gate)
    ups = from_sides(up)
    gate_far = turn(gates[0], 1)
    up_far = turn(ups[1], -1)
    downs, at = [], 0
    for i, width in enumerate(PIECES):
        part = down[:, at : at + width]
        at += width
        sides = from_sides(part)
        far = turn(sides[i % 2], 1 - 2 * (i % 2))
        downs.append((part, *sides, far))

    outgoing = pl.pallas_call(
        lambda *refs: dispatch_kernel(*refs, expert_count=expert_count, slot_cap=slot_cap),
        out_shape=jax.ShapeDtypeStruct((slots, model_width), jnp.bfloat16),
        in_specs=[vmem] * 3,
        out_specs=vmem,
        name="dispatch",
    )(ids_t, expert_input, norm_gain[None])
    arrived = lax.all_to_all(
        outgoing.reshape(expert_count, slot_cap, model_width), "ep", 0, 0, tiled=True
    ).reshape(slots, model_width)
    mix = pl.pallas_call(
        lambda *refs: mix_kernel(*refs, expert_count=expert_count, slot_cap=slot_cap),
        out_shape=jax.ShapeDtypeStruct((2 * token_count, slots), jnp.bfloat16),
        in_specs=[vmem] * 2,
        out_specs=vmem,
        name="mix",
    )(ids_t, weight_t)

    tap_span = CONV - 1
    product = in_gate.astype(jnp.float32) * conv_input.astype(jnp.float32)
    devices = expert_count * lax.axis_size("tp")
    earlier = lax.ppermute(
        product[row_count - tap_span :], ("ep", "tp"), [(i, i + 1) for i in range(devices - 1)]
    )
    padded = jnp.concatenate([earlier, product], axis=0)
    taps = conv_taps.astype(jnp.float32)
    smoothed = sum(padded[j : j + row_count] * taps[j] for j in range(CONV))
    gated = (out_gate.astype(jnp.float32) * smoothed).astype(jnp.bfloat16)

    hidden = hidden_of(arrived, list(zip((gate, *gates), (up, *ups))))
    hidden += hidden_of(arrived, [(gate_far, up_far)])

    results, at = [], 0
    for chunk, block in CHUNKS:
        result = down_of(hidden, [downs[piece] for piece in chunk], block)
        width = result.shape[1]
        back = lax.all_to_all(result.reshape(expert_count, slot_cap, width), "ep", 0, 0, tiled=True)
        results = [combine(mix, back.reshape(slots, width), at, model_width, results)]
        at += width

    gated_sides = from_sides(gated)
    gated_far = from_opposite(*gated_sides)
    mixer_out = pl.pallas_call(
        mixer_kernel,
        out_shape=jax.ShapeDtypeStruct((4 * row_count, mixer_weight.shape[1]), jnp.bfloat16),
        in_specs=[pl.BlockSpec(memory_space=pltpu.SMEM)] + [vmem] * 6,
        out_specs=vmem,
        name="mixer",
    )(lax.axis_index("tp").reshape(1), gated, *gated_sides, *gated_far, mixer_weight)

    return (mixer_out, results[0])


def solution(mesh):
    return jax.shard_map(
        local,
        mesh=mesh,
        in_specs=(
            P(("ep", "tp"), None),
            P(("ep", "tp"), None),
            P(("ep", "tp"), None),
            P(),
            P(None, "tp"),
            P(("ep", "tp"), None),
            P(),
            P("ep", None, "tp"),
            P("ep", None, "tp"),
            P("ep", "tp", None),
            P(("ep", "tp"), None),
            P(("ep", "tp"), None),
        ),
        out_specs=(P("ep", "tp"), P(("ep", "tp"), None)),
        check_vma=False,
    )
```

```python
import jax
import jax.numpy as jnp
from jax import lax
from jax.experimental import pallas as pl
from jax.experimental.pallas import tpu as pltpu
from jax.sharding import PartitionSpec as P


CONV = 3
NORM_EPS = 1e-06
PIECES = (384, 384, 768, 512)
CHUNKS = ((0, 1), (2, 3))
COLUMNS = 256
MIB = 1 << 20


def turn(value, steps):
    count = lax.axis_size("tp")
    pairs = [(source, (source + steps) % count) for source in range(count)]
    return lax.ppermute(value, "tp", pairs)


def from_sides(value):
    return turn(value, 1), turn(value, -1)


def from_opposite(left, right):
    half = left.shape[0] // 2
    return turn(left[:half], 1), turn(right[half:], -1)


def slot_table(ids, expert_count, slot_cap):
    tokens = ids.shape[1]
    expert = lax.broadcasted_iota(jnp.int32, (expert_count, tokens), 0)
    chosen = [ids[k : k + 1] == expert for k in range(ids.shape[0])]
    member = jnp.where(chosen[0] | chosen[1], 1.0, 0.0).astype(jnp.bfloat16)
    row = lax.broadcasted_iota(jnp.int32, (tokens, tokens), 0)
    column = lax.broadcasted_iota(jnp.int32, (tokens, tokens), 1)
    earlier = jnp.where(row < column, 1.0, 0.0).astype(jnp.bfloat16)
    before = jnp.dot(member, earlier, preferred_element_type=jnp.float32).astype(jnp.int32)
    shape = (expert_count, slot_cap, tokens)
    slot = lax.broadcasted_iota(jnp.int32, shape, 1)
    here = jnp.broadcast_to(before[:, None, :], shape) == slot
    return [
        jnp.where(here, jnp.broadcast_to(jnp.where(c, 1.0, 0.0)[:, None, :], shape), 0.0).reshape(
            expert_count * slot_cap, tokens
        )
        for c in chosen
    ]


def dispatch_kernel(ids_ref, input_ref, gain_ref, out_ref, *, expert_count, slot_cap):
    wide = input_ref[...].astype(jnp.float32)
    inv_norm = lax.rsqrt(jnp.mean(wide * wide, axis=1, keepdims=True) + NORM_EPS)
    normed = (wide * inv_norm * gain_ref[...]).astype(jnp.bfloat16)
    table = sum(slot_table(ids_ref[...], expert_count, slot_cap)).astype(jnp.bfloat16)
    out_ref[...] = jnp.dot(table, normed, preferred_element_type=jnp.float32).astype(jnp.bfloat16)


def mix_kernel(ids_ref, weight_ref, out_ref, *, expert_count, slot_cap):
    weight = weight_ref[...]
    tokens = weight.shape[1]
    share = weight / (weight[0:1] + weight[1:2])
    tables = slot_table(ids_ref[...], expert_count, slot_cap)
    mix = (tables[0] * share[0:1] + tables[1] * share[1:2]).T
    high = mix.astype(jnp.bfloat16)
    out_ref[:tokens] = high
    out_ref[tokens:] = (mix - high.astype(jnp.float32)).astype(jnp.bfloat16)


def combine_kernel(mix_ref, *refs):
    chunks, out_ref, made, sent = refs[:-3], refs[-3], refs[-2], refs[-1]
    tokens, at, copies = made.shape[0], 0, []
    for chunk in chunks:
        for first in range(0, chunk.shape[1], COLUMNS):
            both = dot32(mix_ref[...], chunk[:, first : first + COLUMNS])
            made[:, at : at + COLUMNS] = (both[:tokens] + both[tokens:]).astype(jnp.bfloat16)
            place = pl.ds(at, COLUMNS)
            copies.append(pltpu.make_async_copy(made.at[:, place], out_ref.at[:, place], sent.at[len(copies)]))
            copies[-1].start()
            at += COLUMNS
    for copy in copies:
        copy.wait()


def hidden_kernel(rows_ref, *refs):
    weights, out_ref = refs[:-1], refs[-1]
    units = weights[0].shape[1]
    for i in range(len(weights) // 2):
        gate = dot32(rows_ref[...], weights[2 * i][...])
        up = dot32(rows_ref[...], weights[2 * i + 1][...])
        out_ref[:, i * units : (i + 1) * units] = (gate / (1.0 + jnp.exp(-gate)) * up).astype(jnp.bfloat16)


def down_kernel(near_ref, far_ref, *refs):
    downs, (out_ref, hidden, weight) = refs[:-3], refs[-3:]
    middle, units, at = near_ref.shape[1], far_ref.shape[1], 0
    hidden[:, :middle] = near_ref[...]
    hidden[:, middle:] = far_ref[...]
    for i in range(0, len(downs), 4):
        width = downs[i].shape[1]
        for k in range(4):
            weight[k * units : (k + 1) * units, at : at + width] = downs[i + k][...]
        at += width
    out_ref[...] = dot32(hidden[...], weight[...]).astype(jnp.bfloat16)


def on_core(kernel, shape, operands, mib, scratch=(), out=pltpu.VMEM):
    return pl.pallas_call(
        kernel,
        out_shape=jax.ShapeDtypeStruct(shape, jnp.bfloat16),
        in_specs=[pl.BlockSpec(memory_space=pltpu.VMEM)] * len(operands),
        out_specs=pl.BlockSpec(memory_space=out),
        scratch_shapes=list(scratch),
        compiler_params=pltpu.CompilerParams(vmem_limit_bytes=mib * MIB),
    )(*operands)


def mixer_kernel(place_ref, own_ref, left_ref, right_ref, first_ref, second_ref, weight_ref, out_ref):
    rows = own_ref.shape[0]
    weight = weight_ref[...]

    def put(ref, steps, offset):
        block = jnp.dot(ref[...], weight, preferred_element_type=jnp.float32).astype(jnp.bfloat16)
        at = ((place_ref[0] + steps) & 3) * rows + offset
        out_ref[pl.ds(pl.multiple_of(at, rows // 2), block.shape[0]), :] = block

    put(own_ref, 0, 0)
    put(left_ref, 3, 0)
    put(right_ref, 1, 0)
    put(first_ref, 2, 0)
    put(second_ref, 2, rows // 2)


def dot32(a, b):
    return jnp.dot(a, b, preferred_element_type=jnp.float32)


def local(
    out_gate,
    in_gate,
    conv_input,
    conv_taps,
    mixer_weight,
    expert_input,
    norm_gain,
    expert_gate,
    expert_up,
    expert_down,
    expert_ids,
    route_weight,
):
    row_count, model_width = in_gate.shape
    token_count = expert_input.shape[0]
    expert_count = lax.axis_size("ep")
    slot_cap = 4 * token_count // expert_count
    slots = expert_count * slot_cap
    vmem = pl.BlockSpec(memory_space=pltpu.VMEM)
    ids_t = expert_ids.T
    weight_t = route_weight.T

    gate, up, down = expert_gate[0], expert_up[0], expert_down[0]
    gates = from_sides(gate)
    ups = from_sides(up)
    gate_far = turn(gates[0], 1)
    up_far = turn(ups[1], -1)
    downs, at = [], 0
    for i, width in enumerate(PIECES):
        part = down[:, at : at + width]
        at += width
        sides = from_sides(part)
        far = turn(sides[i % 2], 1 - 2 * (i % 2))
        downs.append((part, *sides, far))

    outgoing = on_core(
        lambda *refs: dispatch_kernel(*refs, expert_count=expert_count, slot_cap=slot_cap),
        (slots, model_width),
        (ids_t, expert_input, norm_gain[None]),
        12,
    )
    arrived = lax.all_to_all(
        outgoing.reshape(expert_count, slot_cap, model_width), "ep", 0, 0, tiled=True
    ).reshape(slots, model_width)
    mix = on_core(
        lambda *refs: mix_kernel(*refs, expert_count=expert_count, slot_cap=slot_cap),
        (2 * token_count, slots),
        (ids_t, weight_t),
        8,
    )

    tap_span = CONV - 1
    product = in_gate.astype(jnp.float32) * conv_input.astype(jnp.float32)
    devices = expert_count * lax.axis_size("tp")
    earlier = lax.ppermute(
        product[row_count - tap_span :], ("ep", "tp"), [(i, i + 1) for i in range(devices - 1)]
    )
    padded = jnp.concatenate([earlier, product], axis=0)
    taps = conv_taps.astype(jnp.float32)
    smoothed = sum(padded[j : j + row_count] * taps[j] for j in range(CONV))
    gated = (out_gate.astype(jnp.float32) * smoothed).astype(jnp.bfloat16)

    units = gate.shape[1]
    near_weights = (gate, up, gates[0], ups[0], gates[1], ups[1])
    near = on_core(hidden_kernel, (slots, 3 * units), (arrived, *near_weights), 12)
    far = on_core(hidden_kernel, (slots, units), (arrived, gate_far, up_far), 8)

    returned = []
    for chunk in CHUNKS:
        width = sum(PIECES[piece] for piece in chunk)
        operands = (near, far, *[d for piece in chunk for d in downs[piece]])
        scratch = (pltpu.VMEM((slots, 4 * units), jnp.bfloat16), pltpu.VMEM((4 * units, width), jnp.bfloat16))
        result = on_core(down_kernel, (slots, width), operands, 14, scratch)
        back = lax.all_to_all(result.reshape(expert_count, slot_cap, width), "ep", 0, 0, tiled=True)
        returned.append(back.reshape(slots, width))

    gated_sides = from_sides(gated)
    gated_far = from_opposite(*gated_sides)
    mixer_out = pl.pallas_call(
        mixer_kernel,
        out_shape=jax.ShapeDtypeStruct((4 * row_count, mixer_weight.shape[1]), jnp.bfloat16),
        in_specs=[pl.BlockSpec(memory_space=pltpu.SMEM)] + [vmem] * 6,
        out_specs=vmem,
        compiler_params=pltpu.CompilerParams(vmem_limit_bytes=8 * MIB),
        name="mixer",
    )(lax.axis_index("tp").reshape(1), gated, *gated_sides, *gated_far, mixer_weight)

    scratch = (
        pltpu.VMEM((token_count, model_width), jnp.bfloat16),
        pltpu.SemaphoreType.DMA((model_width // COLUMNS,)),
    )
    experts_out = on_core(combine_kernel, (token_count, model_width), (mix, *returned), 8, scratch, pl.ANY)
    return (mixer_out, experts_out)


def solution(mesh):
    return jax.shard_map(
        local,
        mesh=mesh,
        in_specs=(
            P(("ep", "tp"), None),
            P(("ep", "tp"), None),
            P(("ep", "tp"), None),
            P(),
            P(None, "tp"),
            P(("ep", "tp"), None),
            P(),
            P("ep", None, "tp"),
            P("ep", None, "tp"),
            P("ep", "tp", None),
            P(("ep", "tp"), None),
            P(("ep", "tp"), None),
        ),
        out_specs=(P("ep", "tp"), P(("ep", "tp"), None)),
        check_vma=False,
    )
```

```python
import jax
import jax.numpy as jnp
from jax import lax
from jax.experimental import pallas as pl
from jax.experimental.pallas import tpu as pltpu
from jax.sharding import PartitionSpec as P


CONV = 3
NORM_EPS = 1e-06
PIECES = (384, 384, 768, 512)
CHUNKS = ((0, 1), (2, 3))
COLUMNS = 256
MIB = 1 << 20


def turn(value, steps):
    count = lax.axis_size("tp")
    pairs = [(source, (source + steps) % count) for source in range(count)]
    return lax.ppermute(value, "tp", pairs)


def from_sides(value):
    return turn(value, 1), turn(value, -1)


def from_opposite(left, right):
    half = left.shape[0] // 2
    return turn(left[:half], 1), turn(right[half:], -1)


def slot_table(ids, expert_count, slot_cap):
    tokens = ids.shape[1]
    expert = lax.broadcasted_iota(jnp.int32, (expert_count, tokens), 0)
    chosen = [ids[k : k + 1] == expert for k in range(ids.shape[0])]
    member = jnp.where(chosen[0] | chosen[1], 1.0, 0.0).astype(jnp.bfloat16)
    row = lax.broadcasted_iota(jnp.int32, (tokens, tokens), 0)
    column = lax.broadcasted_iota(jnp.int32, (tokens, tokens), 1)
    earlier = jnp.where(row < column, 1.0, 0.0).astype(jnp.bfloat16)
    before = jnp.dot(member, earlier, preferred_element_type=jnp.float32).astype(jnp.int32)
    shape = (expert_count, slot_cap, tokens)
    slot = lax.broadcasted_iota(jnp.int32, shape, 1)
    here = jnp.broadcast_to(before[:, None, :], shape) == slot
    return [
        jnp.where(here, jnp.broadcast_to(jnp.where(c, 1.0, 0.0)[:, None, :], shape), 0.0).reshape(
            expert_count * slot_cap, tokens
        )
        for c in chosen
    ]


def dispatch_kernel(ids_ref, input_ref, gain_ref, out_ref, *, expert_count, slot_cap):
    wide = input_ref[...].astype(jnp.float32)
    inv_norm = lax.rsqrt(jnp.mean(wide * wide, axis=1, keepdims=True) + NORM_EPS)
    normed = (wide * inv_norm * gain_ref[...]).astype(jnp.bfloat16)
    table = sum(slot_table(ids_ref[...], expert_count, slot_cap)).astype(jnp.bfloat16)
    out_ref[...] = jnp.dot(table, normed, preferred_element_type=jnp.float32).astype(jnp.bfloat16)


def mix_kernel(ids_ref, weight_ref, out_ref, *, expert_count, slot_cap):
    weight = weight_ref[...]
    tokens = weight.shape[1]
    share = weight / (weight[0:1] + weight[1:2])
    tables = slot_table(ids_ref[...], expert_count, slot_cap)
    mix = (tables[0] * share[0:1] + tables[1] * share[1:2]).T
    high = mix.astype(jnp.bfloat16)
    out_ref[:tokens] = high
    out_ref[tokens:] = (mix - high.astype(jnp.float32)).astype(jnp.bfloat16)


def combine_kernel(mix_ref, *refs):
    chunks, out_ref, made, sent = refs[:-3], refs[-3], refs[-2], refs[-1]
    tokens, at, copies = made.shape[0], 0, []
    for chunk in chunks:
        for first in range(0, chunk.shape[1], COLUMNS):
            both = dot32(mix_ref[...], chunk[:, first : first + COLUMNS])
            made[:, at : at + COLUMNS] = (both[:tokens] + both[tokens:]).astype(jnp.bfloat16)
            place = pl.ds(at, COLUMNS)
            copies.append(pltpu.make_async_copy(made.at[:, place], out_ref.at[:, place], sent.at[len(copies)]))
            copies[-1].start()
            at += COLUMNS
    for copy in copies:
        copy.wait()


def fetch(pairs, sems):
    copies = [pltpu.make_async_copy(s, t, sems.at[i]) for i, (s, t) in enumerate(pairs)]
    for copy in copies:
        copy.start()
    return copies


def hidden_kernel(rows_ref, *refs, count):
    weights, (out_ref, here, sems) = refs[: 2 * count], refs[2 * count :]
    depth, units = weights[0].shape
    half = depth // 2
    parts = [(i, pl.ds(s * half, half)) for shard in range(count) for s in (0, 1) for i in (2 * shard, 2 * shard + 1)]
    copies = fetch([(weights[i].at[p], here.at[i, p]) for i, p in parts], sems)
    for shard in range(count):
        sums = [0.0, 0.0]
        for s in (0, 1):
            for k in (0, 1):
                copies[4 * shard + 2 * s + k].wait()
            rows = rows_ref[:, s * half : (s + 1) * half]
            sums = [total + dot32(rows, here[2 * shard + k, pl.ds(s * half, half)]) for k, total in enumerate(sums)]
        gate, up = sums
        out_ref[:, shard * units : (shard + 1) * units] = (gate / (1.0 + jnp.exp(-gate)) * up).astype(jnp.bfloat16)


def stack_kernel(*refs, widths):
    pieces, (out_ref, sems) = refs[:-2], refs[-2:]
    units, at, pairs = pieces[0].shape[0], 0, []
    for i, width in enumerate(widths):
        for k in range(3):
            pairs.append((pieces[3 * i + k], out_ref.at[pl.ds(k * units, units), pl.ds(at, width)]))
        at += width
    for copy in fetch(pairs, sems):
        copy.wait()


def down_kernel(near_ref, far_ref, stacked_ref, *refs):
    pieces, (out_ref, far_weight, made, came, sent) = refs[:-5], refs[-5:]
    at, pairs, copies = 0, [], []
    for piece in pieces:
        pairs.append((piece, far_weight.at[:, pl.ds(at, piece.shape[1])]))
        at += piece.shape[1]
    for copy in fetch(pairs, came):
        copy.wait()
    for i in range(at // COLUMNS):
        place = pl.ds(i * COLUMNS, COLUMNS)
        total = dot32(near_ref[...], stacked_ref[:, place]) + dot32(far_ref[...], far_weight[:, place])
        made[:, place] = total.astype(jnp.bfloat16)
        copies.append(pltpu.make_async_copy(made.at[:, place], out_ref.at[:, place], sent.at[i]))
        copies[-1].start()
    for copy in copies:
        copy.wait()


def on_core(kernel, shape, operands, mib, scratch=(), out=pltpu.VMEM, away=0):
    count = len(operands) - away
    return pl.pallas_call(
        kernel,
        out_shape=jax.ShapeDtypeStruct(shape, jnp.bfloat16),
        in_specs=[pl.BlockSpec(memory_space=pltpu.VMEM)] * count + [pl.BlockSpec(memory_space=pltpu.HBM)] * away,
        out_specs=pl.BlockSpec(memory_space=out),
        scratch_shapes=list(scratch),
        compiler_params=pltpu.CompilerParams(vmem_limit_bytes=mib * MIB),
    )(*operands)


def mixer_kernel(place_ref, own_ref, left_ref, right_ref, first_ref, second_ref, weight_ref, out_ref):
    rows = own_ref.shape[0]
    weight = weight_ref[...]

    def put(ref, steps, offset):
        block = jnp.dot(ref[...], weight, preferred_element_type=jnp.float32).astype(jnp.bfloat16)
        at = ((place_ref[0] + steps) & 3) * rows + offset
        out_ref[pl.ds(pl.multiple_of(at, rows // 2), block.shape[0]), :] = block

    put(own_ref, 0, 0)
    put(left_ref, 3, 0)
    put(right_ref, 1, 0)
    put(first_ref, 2, 0)
    put(second_ref, 2, rows // 2)


def dot32(a, b):
    return jnp.dot(a, b, preferred_element_type=jnp.float32)


def local(
    out_gate,
    in_gate,
    conv_input,
    conv_taps,
    mixer_weight,
    expert_input,
    norm_gain,
    expert_gate,
    expert_up,
    expert_down,
    expert_ids,
    route_weight,
):
    row_count, model_width = in_gate.shape
    token_count = expert_input.shape[0]
    expert_count = lax.axis_size("ep")
    slot_cap = 4 * token_count // expert_count
    slots = expert_count * slot_cap
    vmem = pl.BlockSpec(memory_space=pltpu.VMEM)
    ids_t = expert_ids.T
    weight_t = route_weight.T

    gate, up, down = expert_gate[0], expert_up[0], expert_down[0]
    gates = from_sides(gate)
    ups = from_sides(up)
    gate_far = turn(gates[0], 1)
    up_far = turn(ups[1], -1)
    downs, at = [], 0
    for i, width in enumerate(PIECES):
        part = down[:, at : at + width]
        at += width
        sides = from_sides(part)
        far = turn(sides[i % 2], 1 - 2 * (i % 2))
        downs.append((part, *sides, far))

    outgoing = on_core(
        lambda *refs: dispatch_kernel(*refs, expert_count=expert_count, slot_cap=slot_cap),
        (slots, model_width),
        (ids_t, expert_input, norm_gain[None]),
        12,
    )
    arrived = lax.all_to_all(
        outgoing.reshape(expert_count, slot_cap, model_width), "ep", 0, 0, tiled=True
    ).reshape(slots, model_width)
    mix = on_core(
        lambda *refs: mix_kernel(*refs, expert_count=expert_count, slot_cap=slot_cap),
        (2 * token_count, slots),
        (ids_t, weight_t),
        8,
    )

    tap_span = CONV - 1
    product = in_gate.astype(jnp.float32) * conv_input.astype(jnp.float32)
    devices = expert_count * lax.axis_size("tp")
    earlier = lax.ppermute(
        product[row_count - tap_span :], ("ep", "tp"), [(i, i + 1) for i in range(devices - 1)]
    )
    padded = jnp.concatenate([earlier, product], axis=0)
    taps = conv_taps.astype(jnp.float32)
    smoothed = sum(padded[j : j + row_count] * taps[j] for j in range(CONV))
    gated = (out_gate.astype(jnp.float32) * smoothed).astype(jnp.bfloat16)

    units = gate.shape[1]

    def hidden(shards):
        weights = [w for shard in shards for w in shard]
        scratch = (
            pltpu.VMEM((len(weights), model_width, units), jnp.bfloat16),
            pltpu.SemaphoreType.DMA((2 * len(weights),)),
        )
        return on_core(
            lambda *refs: hidden_kernel(*refs, count=len(shards)),
            (slots, len(shards) * units),
            (arrived, *weights),
            4 * len(shards) + 6,
            scratch,
            away=len(weights),
        )

    near = hidden(((gate, up), (gates[0], ups[0]), (gates[1], ups[1])))
    far = hidden(((gate_far, up_far),))

    returned = []
    for chunk in CHUNKS:
        widths = [PIECES[piece] for piece in chunk]
        width = sum(widths)
        sides = [d for piece in chunk for d in downs[piece][:3]]
        stacked = on_core(
            lambda *refs, widths=widths: stack_kernel(*refs, widths=widths),
            (3 * units, width),
            sides,
            6,
            (pltpu.SemaphoreType.DMA((len(sides),)),),
            away=len(sides),
        )
        scratch = (
            pltpu.VMEM((units, width), jnp.bfloat16),
            pltpu.VMEM((slots, width), jnp.bfloat16),
            pltpu.SemaphoreType.DMA((len(chunk),)),
            pltpu.SemaphoreType.DMA((width // COLUMNS,)),
        )
        operands = (near, far, stacked, *[downs[piece][3] for piece in chunk])
        result = on_core(down_kernel, (slots, width), operands, 12, scratch, pltpu.HBM, away=len(chunk))
        back = lax.all_to_all(result.reshape(expert_count, slot_cap, width), "ep", 0, 0, tiled=True)
        returned.append(back.reshape(slots, width))

    gated_sides = from_sides(gated)
    gated_far = from_opposite(*gated_sides)
    mixer_out = pl.pallas_call(
        mixer_kernel,
        out_shape=jax.ShapeDtypeStruct((4 * row_count, mixer_weight.shape[1]), jnp.bfloat16),
        in_specs=[pl.BlockSpec(memory_space=pltpu.SMEM)] + [vmem] * 6,
        out_specs=vmem,
        compiler_params=pltpu.CompilerParams(vmem_limit_bytes=8 * MIB),
        name="mixer",
    )(lax.axis_index("tp").reshape(1), gated, *gated_sides, *gated_far, mixer_weight)

    scratch = (
        pltpu.VMEM((token_count, model_width), jnp.bfloat16),
        pltpu.SemaphoreType.DMA((model_width // COLUMNS,)),
    )
    experts_out = on_core(combine_kernel, (token_count, model_width), (mix, *returned), 8, scratch, pltpu.HBM)
    return (mixer_out, experts_out)


def solution(mesh):
    return jax.shard_map(
        local,
        mesh=mesh,
        in_specs=(
            P(("ep", "tp"), None),
            P(("ep", "tp"), None),
            P(("ep", "tp"), None),
            P(),
            P(None, "tp"),
            P(("ep", "tp"), None),
            P(),
            P("ep", None, "tp"),
            P("ep", None, "tp"),
            P("ep", "tp", None),
            P(("ep", "tp"), None),
            P(("ep", "tp"), None),
        ),
        out_specs=(P("ep", "tp"), P(("ep", "tp"), None)),
        check_vma=False,
    )
```

```python
import jax
import jax.numpy as jnp
from jax import lax
from jax.experimental import pallas as pl
from jax.experimental.pallas import tpu as pltpu
from jax.sharding import PartitionSpec as P


CONV = 3
NORM_EPS = 1e-06
PIECES = (512, 512, 512, 512)
CHUNKS = ((0, 1), (2, 3))
COLUMNS = 256
MIB = 1 << 20


def turn(value, steps):
    count = lax.axis_size("tp")
    pairs = [(source, (source + steps) % count) for source in range(count)]
    return lax.ppermute(value, "tp", pairs)


def from_sides(value):
    return turn(value, 1), turn(value, -1)


def from_opposite(left, right):
    half = left.shape[0] // 2
    return turn(left[:half], 1), turn(right[half:], -1)


def slot_table(ids, expert_count, slot_cap, number=lambda i: i):
    tokens = ids.shape[1]
    expert = number(lax.broadcasted_iota(jnp.int32, (expert_count, tokens), 0))
    chosen = [ids[k : k + 1] == expert for k in range(ids.shape[0])]
    member = jnp.where(chosen[0] | chosen[1], 1.0, 0.0).astype(jnp.bfloat16)
    row = lax.broadcasted_iota(jnp.int32, (tokens, tokens), 0)
    column = lax.broadcasted_iota(jnp.int32, (tokens, tokens), 1)
    earlier = jnp.where(row < column, 1.0, 0.0).astype(jnp.bfloat16)
    before = jnp.dot(member, earlier, preferred_element_type=jnp.float32).astype(jnp.int32)
    shape = (expert_count, slot_cap, tokens)
    slot = lax.broadcasted_iota(jnp.int32, shape, 1)
    here = jnp.broadcast_to(before[:, None, :], shape) == slot
    return [
        jnp.where(here, jnp.broadcast_to(jnp.where(c, 1.0, 0.0)[:, None, :], shape), 0.0).reshape(
            expert_count * slot_cap, tokens
        )
        for c in chosen
    ]


def dispatch_kernel(ids_ref, input_ref, gain_ref, out_ref, *, expert_count, slot_cap):
    wide = input_ref[...].astype(jnp.float32)
    inv_norm = lax.rsqrt(jnp.mean(wide * wide, axis=1, keepdims=True) + NORM_EPS)
    normed = (wide * inv_norm * gain_ref[...]).astype(jnp.bfloat16)
    table = sum(slot_table(ids_ref[...], expert_count, slot_cap)).astype(jnp.bfloat16)
    out_ref[...] = jnp.dot(table, normed, preferred_element_type=jnp.float32).astype(jnp.bfloat16)


def mix_kernel(place_ref, ids_ref, weight_ref, out_ref, *, expert_count, slot_cap):
    weight, ids = weight_ref[...], ids_ref[...]
    tokens = weight.shape[1]
    share = weight / (weight[0:1] + weight[1:2])
    z, member = place_ref[0], place_ref[1]

    def stepped(i):
        return ((z - (i & 7)) & 7) * 8 + (member ^ lax.shift_right_logical(i, 3))

    for t, number in enumerate((stepped, lambda i: i)):
        tables = slot_table(ids, expert_count, slot_cap, number)
        mix = (tables[0] * share[0:1] + tables[1] * share[1:2]).T
        high = mix.astype(jnp.bfloat16)
        out_ref[2 * t * tokens : (2 * t + 1) * tokens] = high
        out_ref[(2 * t + 1) * tokens : (2 * t + 2) * tokens] = (mix - high.astype(jnp.float32)).astype(jnp.bfloat16)


def early_kernel(mix_ref, *refs):
    blocks, (out_ref, rows) = refs[:-2], refs[-2:]
    tokens, count = out_ref.shape[0], blocks[0].shape[0]
    for i, block in enumerate(blocks):
        rows[i * count : (i + 1) * count, :] = block[...]
    both = dot32(mix_ref[: 2 * tokens], rows[...])
    out_ref[...] = (both[:tokens] + both[tokens:]).astype(jnp.bfloat16)


def combine_kernel(mix_ref, early_ref, rows_ref, out_ref, made, sent):
    tokens, at = early_ref.shape
    copies = [pltpu.make_async_copy(early_ref, out_ref.at[:, pl.ds(0, at)], sent.at[0])]
    copies[0].start()
    for first in range(0, rows_ref.shape[1], COLUMNS):
        both = dot32(mix_ref[2 * tokens :], rows_ref[:, first : first + COLUMNS])
        made[:, first : first + COLUMNS] = (both[:tokens] + both[tokens:]).astype(jnp.bfloat16)
        here, there = made.at[:, pl.ds(first, COLUMNS)], out_ref.at[:, pl.ds(at + first, COLUMNS)]
        copies.append(pltpu.make_async_copy(here, there, sent.at[len(copies)]))
        copies[-1].start()
    for copy in copies:
        copy.wait()


def spread_kernel(place_ref, *refs):
    planes, blocks, sems = refs[:8], refs[8:16], refs[16]
    rows, copies = planes[0].shape[0] // 8, []
    for k in range(8):
        start = pl.multiple_of((place_ref[1] ^ k) * rows, rows)
        for z in range(8):
            here, there = planes[z].at[pl.ds(start, rows)], blocks[k].at[pl.ds(z * rows, rows)]
            copies.append(pltpu.make_async_copy(here, there, sems.at[len(copies)]))
            copies[-1].start()
    for copy in copies:
        copy.wait()


def fetch(pairs, sems):
    copies = [pltpu.make_async_copy(s, t, sems.at[i]) for i, (s, t) in enumerate(pairs)]
    for copy in copies:
        copy.start()
    return copies


def hidden_kernel(rows_ref, *refs, count):
    weights, (out_ref, here, sems) = refs[: 2 * count], refs[2 * count :]
    depth, units = weights[0].shape
    half = depth // 2
    parts = [(i, pl.ds(s * half, half)) for shard in range(count) for s in (0, 1) for i in (2 * shard, 2 * shard + 1)]
    fetch([(weights[i].at[p], here.at[i, p]) for i, p in parts], sems)

    def shard_of(shard, _):
        sums = [0.0, 0.0]
        for s in (0, 1):
            part = pl.ds(s * half, half)
            for k in (0, 1):
                there = here.at[2 * shard + k, part]
                pltpu.make_async_copy(there, there, sems.at[4 * shard + 2 * s + k]).wait()
            rows = rows_ref[:, s * half : (s + 1) * half]
            sums = [total + dot32(rows, here[2 * shard + k, part]) for k, total in enumerate(sums)]
        gate, up = sums
        columns = pl.ds(pl.multiple_of(shard * units, units), units)
        out_ref[:, columns] = (gate / (1.0 + jnp.exp(-gate)) * up).astype(jnp.bfloat16)
        return _

    lax.fori_loop(0, count, shard_of, 0)


def stack_kernel(*refs, widths):
    pieces, (out_ref, sems) = refs[:-2], refs[-2:]
    units, at, pairs = pieces[0].shape[0], 0, []
    for i, width in enumerate(widths):
        for k in range(3):
            pairs.append((pieces[3 * i + k], out_ref.at[pl.ds(k * units, units), pl.ds(at, width)]))
        at += width
    for copy in fetch(pairs, sems):
        copy.wait()


def down_kernel(place_ref, near_ref, far_ref, stacked_ref, *refs, planes):
    pieces, outs, (far_weight, made, came, sent) = refs[:2], refs[2:-4], refs[-4:]
    at, pairs, copies = 0, [], []
    for piece in pieces:
        pairs.append((piece, far_weight.at[:, pl.ds(at, piece.shape[1])]))
        at += piece.shape[1]
    for copy in fetch(pairs, came):
        copy.wait()

    def block(i, _):
        place = pl.ds(pl.multiple_of(i * COLUMNS, COLUMNS), COLUMNS)
        total = dot32(near_ref[...], stacked_ref[:, place]) + dot32(far_ref[...], far_weight[:, place])
        made[:, place] = total.astype(jnp.bfloat16)
        if not planes:
            pltpu.make_async_copy(made.at[:, place], outs[0].at[:, place], sent.at[i]).start()
        return _

    lax.fori_loop(0, at // COLUMNS, block, 0)
    for i in range(0 if planes else at // COLUMNS):
        place = pl.ds(i * COLUMNS, COLUMNS)
        copies.append(pltpu.make_async_copy(made.at[:, place], outs[0].at[:, place], sent.at[i]))
    if planes:
        rows = outs[0].shape[0]
        starts = [pl.multiple_of(((place_ref[0] + d) & 7) * rows, rows) for d in range(8)]
        copies = fetch([(made.at[pl.ds(s, rows)], out) for s, out in zip(starts, outs)], sent)
    for copy in copies:
        copy.wait()


def on_core(kernel, shape, operands, mib, scratch=(), out=pltpu.VMEM, away=0, scalars=0, several=0):
    count = len(operands) - away - scalars
    space = [pltpu.SMEM] * scalars + [pltpu.VMEM] * count + [pltpu.HBM] * away
    result, placed = jax.ShapeDtypeStruct(shape, jnp.bfloat16), pl.BlockSpec(memory_space=out)
    return pl.pallas_call(
        kernel,
        out_shape=[result] * several if several else result,
        in_specs=[pl.BlockSpec(memory_space=s) for s in space],
        out_specs=[placed] * several if several else placed,
        scratch_shapes=list(scratch),
        compiler_params=pltpu.CompilerParams(vmem_limit_bytes=mib * MIB),
    )(*operands)


def mixer_kernel(place_ref, own_ref, left_ref, right_ref, first_ref, second_ref, weight_ref, out_ref):
    rows = own_ref.shape[0]
    weight = weight_ref[...]

    def put(ref, steps, offset):
        block = jnp.dot(ref[...], weight, preferred_element_type=jnp.float32).astype(jnp.bfloat16)
        at = ((place_ref[0] + steps) & 3) * rows + offset
        out_ref[pl.ds(pl.multiple_of(at, rows // 2), block.shape[0]), :] = block

    put(own_ref, 0, 0)
    put(left_ref, 3, 0)
    put(right_ref, 1, 0)
    put(first_ref, 2, 0)
    put(second_ref, 2, rows // 2)


def dot32(a, b):
    return jnp.dot(a, b, preferred_element_type=jnp.float32)


def local(
    out_gate,
    in_gate,
    conv_input,
    conv_taps,
    mixer_weight,
    expert_input,
    norm_gain,
    expert_gate,
    expert_up,
    expert_down,
    expert_ids,
    route_weight,
):
    row_count, model_width = in_gate.shape
    token_count = expert_input.shape[0]
    expert_count = lax.axis_size("ep")
    slot_cap = 4 * token_count // expert_count
    slots = expert_count * slot_cap
    vmem = pl.BlockSpec(memory_space=pltpu.VMEM)
    ids_t = expert_ids.T
    weight_t = route_weight.T

    gate, up, down = expert_gate[0], expert_up[0], expert_down[0]
    gates = from_sides(gate)
    ups = from_sides(up)
    gate_far = turn(gates[0], 1)
    up_far = turn(ups[1], -1)
    downs, at = [], 0
    for i, width in enumerate(PIECES):
        part = down[:, at : at + width]
        at += width
        sides = from_sides(part)
        far = turn(sides[i % 2], 1 - 2 * (i % 2))
        downs.append((part, *sides, far))

    outgoing = on_core(
        lambda *refs: dispatch_kernel(*refs, expert_count=expert_count, slot_cap=slot_cap),
        (slots, model_width),
        (ids_t, expert_input, norm_gain[None]),
        12,
    )
    arrived = lax.all_to_all(
        outgoing.reshape(expert_count, slot_cap, model_width), "ep", 0, 0, tiled=True
    ).reshape(slots, model_width)
    ep = lax.axis_index("ep")
    place = jnp.stack([ep // 8, ep % 8]).astype(jnp.int32)
    mix = on_core(
        lambda *refs: mix_kernel(*refs, expert_count=expert_count, slot_cap=slot_cap),
        (4 * token_count, slots),
        (place, ids_t, weight_t),
        8,
        scalars=1,
    )

    tap_span = CONV - 1
    product = in_gate.astype(jnp.float32) * conv_input.astype(jnp.float32)
    devices = expert_count * lax.axis_size("tp")
    earlier = lax.ppermute(
        product[row_count - tap_span :], ("ep", "tp"), [(i, i + 1) for i in range(devices - 1)]
    )
    padded = jnp.concatenate([earlier, product], axis=0)
    taps = conv_taps.astype(jnp.float32)
    smoothed = sum(padded[j : j + row_count] * taps[j] for j in range(CONV))
    gated = (out_gate.astype(jnp.float32) * smoothed).astype(jnp.bfloat16)

    units = gate.shape[1]

    def hidden(shards):
        weights = [w for shard in shards for w in shard]
        scratch = (
            pltpu.VMEM((len(weights), model_width, units), jnp.bfloat16),
            pltpu.SemaphoreType.DMA((2 * len(weights),)),
        )
        return on_core(
            lambda *refs: hidden_kernel(*refs, count=len(shards)),
            (slots, len(shards) * units),
            (arrived, *weights),
            4 * len(shards) + 6,
            scratch,
            away=len(weights),
        )

    near = hidden(((gate, up), (gates[0], ups[0]), (gates[1], ups[1])))
    far = hidden(((gate_far, up_far),))

    results = []
    for i, chunk in enumerate(CHUNKS):
        widths = [PIECES[piece] for piece in chunk]
        width = sum(widths)
        sides = [d for piece in chunk for d in downs[piece][:3]]
        stacked = on_core(
            lambda *refs, widths=widths: stack_kernel(*refs, widths=widths),
            (3 * units, width),
            sides,
            6,
            (pltpu.SemaphoreType.DMA((len(sides),)),),
            away=len(sides),
        )
        scratch = (
            pltpu.VMEM((units, width), jnp.bfloat16),
            pltpu.VMEM((slots, width), jnp.bfloat16),
            pltpu.SemaphoreType.DMA((2,)),
            pltpu.SemaphoreType.DMA((8,)),
        )
        results.append(
            on_core(
                lambda *refs, i=i: down_kernel(*refs, planes=i == 0),
                (slots // 8, width) if i == 0 else (slots, width),
                (place, near, far, stacked, *[downs[piece][3] for piece in chunk]),
                12,
                scratch,
                pltpu.HBM,
                away=2,
                scalars=1,
                several=8 if i == 0 else 0,
            )
        )

    planes, last = results
    width = last.shape[1]

    def hop(value, target):
        return lax.ppermute(value, "ep", [(p, target(p // 8, p % 8)) for p in range(expert_count)])

    planes = [planes[0]] + [hop(planes[d], lambda z, m, d=d: (z + d) % 8 * 8 + m) for d in range(1, 8)]
    blocks = on_core(
        spread_kernel,
        planes[0].shape,
        (place, *planes),
        4,
        (pltpu.SemaphoreType.DMA((64,)),),
        pltpu.HBM,
        away=8,
        scalars=1,
        several=8,
    )
    blocks = [blocks[0]] + [hop(blocks[k], lambda z, m, k=k: z * 8 + (m ^ k)) for k in range(1, 8)]
    early = on_core(
        early_kernel,
        (token_count, planes[0].shape[1]),
        (mix, *blocks),
        8,
        (pltpu.VMEM((slots, planes[0].shape[1]), jnp.bfloat16),),
    )
    back = lax.all_to_all(last.reshape(expert_count, slot_cap, width), "ep", 0, 0, tiled=True)
    back = back.reshape(slots, width)

    gated_sides = from_sides(gated)
    gated_far = from_opposite(*gated_sides)
    mixer_out = pl.pallas_call(
        mixer_kernel,
        out_shape=jax.ShapeDtypeStruct((4 * row_count, mixer_weight.shape[1]), jnp.bfloat16),
        in_specs=[pl.BlockSpec(memory_space=pltpu.SMEM)] + [vmem] * 6,
        out_specs=vmem,
        compiler_params=pltpu.CompilerParams(vmem_limit_bytes=8 * MIB),
        name="mixer",
    )(lax.axis_index("tp").reshape(1), gated, *gated_sides, *gated_far, mixer_weight)

    scratch = (pltpu.VMEM((token_count, width), jnp.bfloat16), pltpu.SemaphoreType.DMA((1 + width // COLUMNS,)))
    experts_out = on_core(combine_kernel, (token_count, model_width), (mix, early, back), 8, scratch, pltpu.HBM)
    return (mixer_out, experts_out)


def solution(mesh):
    return jax.shard_map(
        local,
        mesh=mesh,
        in_specs=(
            P(("ep", "tp"), None),
            P(("ep", "tp"), None),
            P(("ep", "tp"), None),
            P(),
            P(None, "tp"),
            P(("ep", "tp"), None),
            P(),
            P("ep", None, "tp"),
            P("ep", None, "tp"),
            P("ep", "tp", None),
            P(("ep", "tp"), None),
            P(("ep", "tp"), None),
        ),
        out_specs=(P("ep", "tp"), P(("ep", "tp"), None)),
        check_vma=False,
    )
```

```python
import jax
import jax.numpy as jnp
from jax import lax
from jax.experimental import pallas as pl
from jax.experimental.pallas import tpu as pltpu
from jax.sharding import PartitionSpec as P


CONV = 3
NORM_EPS = 1e-06
PIECES = (384, 384, 768, 512)
CHUNKS = ((0, 1), (2, 3))
COLUMNS = 256
MIB = 1 << 20
DOWN_MIB = 12


def turn(value, steps):
    count = lax.axis_size("tp")
    pairs = [(source, (source + steps) % count) for source in range(count)]
    return lax.ppermute(value, "tp", pairs)


def from_sides(value):
    return turn(value, 1), turn(value, -1)


def from_opposite(left, right):
    half = left.shape[0] // 2
    return turn(left[:half], 1), turn(right[half:], -1)


def slot_table(ids, expert_count, slot_cap):
    tokens = ids.shape[1]
    expert = lax.broadcasted_iota(jnp.int32, (expert_count, tokens), 0)
    chosen = [ids[k : k + 1] == expert for k in range(ids.shape[0])]
    member = jnp.where(chosen[0] | chosen[1], 1.0, 0.0).astype(jnp.bfloat16)
    row = lax.broadcasted_iota(jnp.int32, (tokens, tokens), 0)
    column = lax.broadcasted_iota(jnp.int32, (tokens, tokens), 1)
    earlier = jnp.where(row < column, 1.0, 0.0).astype(jnp.bfloat16)
    before = jnp.dot(member, earlier, preferred_element_type=jnp.float32).astype(jnp.int32)
    shape = (expert_count, slot_cap, tokens)
    slot = lax.broadcasted_iota(jnp.int32, shape, 1)
    here = jnp.broadcast_to(before[:, None, :], shape) == slot
    return [
        jnp.where(here, jnp.broadcast_to(jnp.where(c, 1.0, 0.0)[:, None, :], shape), 0.0).reshape(
            expert_count * slot_cap, tokens
        )
        for c in chosen
    ]


def dispatch_kernel(ids_ref, input_ref, gain_ref, out_ref, *, expert_count, slot_cap):
    wide = input_ref[...].astype(jnp.float32)
    inv_norm = lax.rsqrt(jnp.mean(wide * wide, axis=1, keepdims=True) + NORM_EPS)
    normed = (wide * inv_norm * gain_ref[...]).astype(jnp.bfloat16)
    table = sum(slot_table(ids_ref[...], expert_count, slot_cap)).astype(jnp.bfloat16)
    out_ref[...] = jnp.dot(table, normed, preferred_element_type=jnp.float32).astype(jnp.bfloat16)


def mix_kernel(ids_ref, weight_ref, out_ref, *, expert_count, slot_cap):
    weight = weight_ref[...]
    tokens = weight.shape[1]
    share = weight / (weight[0:1] + weight[1:2])
    tables = slot_table(ids_ref[...], expert_count, slot_cap)
    mix = (tables[0] * share[0:1] + tables[1] * share[1:2]).T
    high = mix.astype(jnp.bfloat16)
    out_ref[:tokens] = high
    out_ref[tokens:] = (mix - high.astype(jnp.float32)).astype(jnp.bfloat16)


def combine_kernel(mix_ref, *refs):
    chunks, out_ref, made, sent = refs[:-3], refs[-3], refs[-2], refs[-1]
    tokens, at, copies = made.shape[0], 0, []
    for chunk in chunks:
        for first in range(0, chunk.shape[1], COLUMNS):
            both = dot32(mix_ref[...], chunk[:, first : first + COLUMNS])
            made[:, at : at + COLUMNS] = (both[:tokens] + both[tokens:]).astype(jnp.bfloat16)
            place = pl.ds(at, COLUMNS)
            copies.append(pltpu.make_async_copy(made.at[:, place], out_ref.at[:, place], sent.at[len(copies)]))
            copies[-1].start()
            at += COLUMNS
    for copy in copies:
        copy.wait()


def fetch(pairs, sems):
    copies = [pltpu.make_async_copy(s, t, sems.at[i]) for i, (s, t) in enumerate(pairs)]
    for copy in copies:
        copy.start()
    return copies


def hidden_kernel(rows_ref, *refs, count):
    weights, (out_ref, here, sems) = refs[: 2 * count], refs[2 * count :]
    depth, units = weights[0].shape
    half = depth // 2
    parts = [(i, pl.ds(s * half, half)) for shard in range(count) for s in (0, 1) for i in (2 * shard, 2 * shard + 1)]
    fetch([(weights[i].at[p], here.at[i, p]) for i, p in parts], sems)

    def shard_of(shard, _):
        sums = [0.0, 0.0]
        for s in (0, 1):
            part = pl.ds(s * half, half)
            for k in (0, 1):
                there = here.at[2 * shard + k, part]
                pltpu.make_async_copy(there, there, sems.at[4 * shard + 2 * s + k]).wait()
            rows = rows_ref[:, s * half : (s + 1) * half]
            sums = [total + dot32(rows, here[2 * shard + k, part]) for k, total in enumerate(sums)]
        gate, up = sums
        columns = pl.ds(pl.multiple_of(shard * units, units), units)
        out_ref[:, columns] = (gate / (1.0 + jnp.exp(-gate)) * up).astype(jnp.bfloat16)
        return _

    lax.fori_loop(0, count, shard_of, 0)


def lead_kernel(near_ref, *refs, widths):
    pieces, (out_ref, stacked, sems) = refs[:-3], refs[-3:]
    units, at, pairs = pieces[0].shape[0], 0, []
    for i, width in enumerate(widths):
        for k in range(3):
            pairs.append((pieces[3 * i + k], stacked.at[pl.ds(k * units, units), pl.ds(at, width)]))
        at += width
    for copy in fetch(pairs, sems):
        copy.wait()

    def block(i, _):
        place = pl.ds(pl.multiple_of(i * COLUMNS, COLUMNS), COLUMNS)
        out_ref[:, place] = dot32(near_ref[...], stacked[:, place])
        return _

    lax.fori_loop(0, at // COLUMNS, block, 0)


def down_kernel(lead_ref, far_ref, *refs):
    pieces, (out_ref, far_weight, made, came, sent) = refs[:-5], refs[-5:]
    at, pairs = 0, []
    for piece in pieces:
        pairs.append((piece, far_weight.at[:, pl.ds(at, piece.shape[1])]))
        at += piece.shape[1]
    for copy in fetch(pairs, came):
        copy.wait()

    def outward(i):
        place = pl.ds(pl.multiple_of(i * COLUMNS, COLUMNS), COLUMNS)
        return place, pltpu.make_async_copy(made.at[:, place], out_ref.at[:, place], sent.at[i])

    def block(i, _):
        place, copy = outward(i)
        made[:, place] = (lead_ref[:, place] + dot32(far_ref[...], far_weight[:, place])).astype(jnp.bfloat16)
        copy.start()
        return _

    lax.fori_loop(0, at // COLUMNS, block, 0)
    for i in range(at // COLUMNS):
        outward(i)[1].wait()


def on_core(kernel, shape, operands, mib, scratch=(), out=pltpu.VMEM, away=0, kind=jnp.bfloat16):
    count = len(operands) - away
    return pl.pallas_call(
        kernel,
        out_shape=jax.ShapeDtypeStruct(shape, kind),
        in_specs=[pl.BlockSpec(memory_space=pltpu.VMEM)] * count + [pl.BlockSpec(memory_space=pltpu.HBM)] * away,
        out_specs=pl.BlockSpec(memory_space=out),
        scratch_shapes=list(scratch),
        compiler_params=pltpu.CompilerParams(vmem_limit_bytes=mib * MIB),
    )(*operands)


def mixer_kernel(place_ref, own_ref, left_ref, right_ref, first_ref, second_ref, weight_ref, out_ref):
    rows = own_ref.shape[0]
    weight = weight_ref[...]

    def put(ref, steps, offset):
        block = jnp.dot(ref[...], weight, preferred_element_type=jnp.float32).astype(jnp.bfloat16)
        at = ((place_ref[0] + steps) & 3) * rows + offset
        out_ref[pl.ds(pl.multiple_of(at, rows // 2), block.shape[0]), :] = block

    put(own_ref, 0, 0)
    put(left_ref, 3, 0)
    put(right_ref, 1, 0)
    put(first_ref, 2, 0)
    put(second_ref, 2, rows // 2)


def dot32(a, b):
    return jnp.dot(a, b, preferred_element_type=jnp.float32)


def local(
    out_gate,
    in_gate,
    conv_input,
    conv_taps,
    mixer_weight,
    expert_input,
    norm_gain,
    expert_gate,
    expert_up,
    expert_down,
    expert_ids,
    route_weight,
):
    row_count, model_width = in_gate.shape
    token_count = expert_input.shape[0]
    expert_count = lax.axis_size("ep")
    slot_cap = 4 * token_count // expert_count
    slots = expert_count * slot_cap
    vmem = pl.BlockSpec(memory_space=pltpu.VMEM)
    ids_t = expert_ids.T
    weight_t = route_weight.T

    gate, up, down = expert_gate[0], expert_up[0], expert_down[0]
    gates = from_sides(gate)
    ups = from_sides(up)
    gate_far = turn(gates[0], 1)
    up_far = turn(ups[1], -1)
    downs, at = [], 0
    for i, width in enumerate(PIECES):
        part = down[:, at : at + width]
        at += width
        sides = from_sides(part)
        far = turn(sides[i % 2], 1 - 2 * (i % 2))
        downs.append((part, *sides, far))

    outgoing = on_core(
        lambda *refs: dispatch_kernel(*refs, expert_count=expert_count, slot_cap=slot_cap),
        (slots, model_width),
        (ids_t, expert_input, norm_gain[None]),
        12,
    )
    arrived = lax.all_to_all(
        outgoing.reshape(expert_count, slot_cap, model_width), "ep", 0, 0, tiled=True
    ).reshape(slots, model_width)
    mix = on_core(
        lambda *refs: mix_kernel(*refs, expert_count=expert_count, slot_cap=slot_cap),
        (2 * token_count, slots),
        (ids_t, weight_t),
        8,
    )

    tap_span = CONV - 1
    product = in_gate.astype(jnp.float32) * conv_input.astype(jnp.float32)
    devices = expert_count * lax.axis_size("tp")
    earlier = lax.ppermute(
        product[row_count - tap_span :], ("ep", "tp"), [(i, i + 1) for i in range(devices - 1)]
    )
    padded = jnp.concatenate([earlier, product], axis=0)
    taps = conv_taps.astype(jnp.float32)
    smoothed = sum(padded[j : j + row_count] * taps[j] for j in range(CONV))
    gated = (out_gate.astype(jnp.float32) * smoothed).astype(jnp.bfloat16)

    units = gate.shape[1]

    def hidden(shards):
        weights = [w for shard in shards for w in shard]
        scratch = (
            pltpu.VMEM((len(weights), model_width, units), jnp.bfloat16),
            pltpu.SemaphoreType.DMA((2 * len(weights),)),
        )
        return on_core(
            lambda *refs: hidden_kernel(*refs, count=len(shards)),
            (slots, len(shards) * units),
            (arrived, *weights),
            4 * len(shards) + 6,
            scratch,
            away=len(weights),
        )

    near = hidden(((gate, up), (gates[0], ups[0]), (gates[1], ups[1])))
    far = hidden(((gate_far, up_far),))

    returned = []
    for chunk in CHUNKS:
        widths = [PIECES[piece] for piece in chunk]
        width = sum(widths)
        sides = [d for piece in chunk for d in downs[piece][:3]]
        lead = on_core(
            lambda *refs, widths=widths: lead_kernel(*refs, widths=widths),
            (slots, width),
            (near, *sides),
            12,
            (pltpu.VMEM((3 * units, width), jnp.bfloat16), pltpu.SemaphoreType.DMA((len(sides),))),
            away=len(sides),
            kind=jnp.float32,
        )
        scratch = (
            pltpu.VMEM((units, width), jnp.bfloat16),
            pltpu.VMEM((slots, width), jnp.bfloat16),
            pltpu.SemaphoreType.DMA((len(chunk),)),
            pltpu.SemaphoreType.DMA((width // COLUMNS,)),
        )
        operands = (lead, far, *[downs[piece][3] for piece in chunk])
        result = on_core(down_kernel, (slots, width), operands, DOWN_MIB, scratch, pltpu.HBM, away=len(chunk))
        back = lax.all_to_all(result.reshape(expert_count, slot_cap, width), "ep", 0, 0, tiled=True)
        returned.append(back.reshape(slots, width))

    gated_sides = from_sides(gated)
    gated_far = from_opposite(*gated_sides)
    mixer_out = pl.pallas_call(
        mixer_kernel,
        out_shape=jax.ShapeDtypeStruct((4 * row_count, mixer_weight.shape[1]), jnp.bfloat16),
        in_specs=[pl.BlockSpec(memory_space=pltpu.SMEM)] + [vmem] * 6,
        out_specs=vmem,
        compiler_params=pltpu.CompilerParams(vmem_limit_bytes=8 * MIB),
        name="mixer",
    )(lax.axis_index("tp").reshape(1), gated, *gated_sides, *gated_far, mixer_weight)

    scratch = (
        pltpu.VMEM((token_count, model_width), jnp.bfloat16),
        pltpu.SemaphoreType.DMA((model_width // COLUMNS,)),
    )
    experts_out = on_core(combine_kernel, (token_count, model_width), (mix, *returned), 8, scratch, pltpu.HBM)
    return (mixer_out, experts_out)


def solution(mesh):
    return jax.shard_map(
        local,
        mesh=mesh,
        in_specs=(
            P(("ep", "tp"), None),
            P(("ep", "tp"), None),
            P(("ep", "tp"), None),
            P(),
            P(None, "tp"),
            P(("ep", "tp"), None),
            P(),
            P("ep", None, "tp"),
            P("ep", None, "tp"),
            P("ep", "tp", None),
            P(("ep", "tp"), None),
            P(("ep", "tp"), None),
        ),
        out_specs=(P("ep", "tp"), P(("ep", "tp"), None)),
        check_vma=False,
    )
```

```python
import jax
import jax.numpy as jnp
from jax import lax
from jax.experimental import pallas as pl
from jax.experimental.pallas import tpu as pltpu
from jax.sharding import PartitionSpec as P


CONV = 3
NORM_EPS = 1e-06
PIECES = (384, 256, 768, 640)
CHUNKS = ((0, 1), (2, 3))
COLUMNS = 256
MIB = 1 << 20
DOWN_MIB = 12


def turn(value, steps):
    count = lax.axis_size("tp")
    pairs = [(source, (source + steps) % count) for source in range(count)]
    return lax.ppermute(value, "tp", pairs)


def from_sides(value):
    return turn(value, 1), turn(value, -1)


def from_opposite(left, right):
    half = left.shape[0] // 2
    return turn(left[:half], 1), turn(right[half:], -1)


def slot_table(ids, expert_count, slot_cap):
    tokens = ids.shape[1]
    expert = lax.broadcasted_iota(jnp.int32, (expert_count, tokens), 0)
    chosen = [ids[k : k + 1] == expert for k in range(ids.shape[0])]
    member = jnp.where(chosen[0] | chosen[1], 1.0, 0.0).astype(jnp.bfloat16)
    row = lax.broadcasted_iota(jnp.int32, (tokens, tokens), 0)
    column = lax.broadcasted_iota(jnp.int32, (tokens, tokens), 1)
    earlier = jnp.where(row < column, 1.0, 0.0).astype(jnp.bfloat16)
    before = jnp.dot(member, earlier, preferred_element_type=jnp.float32).astype(jnp.int32)
    shape = (expert_count, slot_cap, tokens)
    slot = lax.broadcasted_iota(jnp.int32, shape, 1)
    here = jnp.broadcast_to(before[:, None, :], shape) == slot
    return [
        jnp.where(here, jnp.broadcast_to(jnp.where(c, 1.0, 0.0)[:, None, :], shape), 0.0).reshape(
            expert_count * slot_cap, tokens
        )
        for c in chosen
    ]


def dispatch_kernel(ids_ref, input_ref, gain_ref, out_ref, *, expert_count, slot_cap):
    wide = input_ref[...].astype(jnp.float32)
    inv_norm = lax.rsqrt(jnp.mean(wide * wide, axis=1, keepdims=True) + NORM_EPS)
    normed = (wide * inv_norm * gain_ref[...]).astype(jnp.bfloat16)
    table = sum(slot_table(ids_ref[...], expert_count, slot_cap)).astype(jnp.bfloat16)
    out_ref[...] = jnp.dot(table, normed, preferred_element_type=jnp.float32).astype(jnp.bfloat16)


def mix_kernel(ids_ref, weight_ref, out_ref, *, expert_count, slot_cap):
    weight = weight_ref[...]
    tokens = weight.shape[1]
    share = weight / (weight[0:1] + weight[1:2])
    tables = slot_table(ids_ref[...], expert_count, slot_cap)
    mix = (tables[0] * share[0:1] + tables[1] * share[1:2]).T
    high = mix.astype(jnp.bfloat16)
    out_ref[:tokens] = high
    out_ref[tokens:] = (mix - high.astype(jnp.float32)).astype(jnp.bfloat16)


def combine_kernel(mix_ref, *refs):
    chunks, out_ref, made, sent = refs[:-3], refs[-3], refs[-2], refs[-1]
    tokens, at, copies = made.shape[0], 0, []
    for chunk in chunks:
        for span in spans(chunk.shape[1]):
            both = dot32(mix_ref[...], chunk[:, span])
            place = pl.ds(at, span.size)
            made[:, place] = (both[:tokens] + both[tokens:]).astype(jnp.bfloat16)
            copies.append(pltpu.make_async_copy(made.at[:, place], out_ref.at[:, place], sent.at[len(copies)]))
            copies[-1].start()
            at += span.size
    for copy in copies:
        copy.wait()


def fetch(pairs, sems):
    copies = [pltpu.make_async_copy(s, t, sems.at[i]) for i, (s, t) in enumerate(pairs)]
    for copy in copies:
        copy.start()
    return copies


def hidden_kernel(rows_ref, *refs, count):
    weights, (out_ref, here, sems) = refs[: 2 * count], refs[2 * count :]
    depth, units = weights[0].shape
    half = depth // 2
    parts = [(i, pl.ds(s * half, half)) for shard in range(count) for s in (0, 1) for i in (2 * shard, 2 * shard + 1)]
    fetch([(weights[i].at[p], here.at[i, p]) for i, p in parts], sems)

    def shard_of(shard, _):
        sums = [0.0, 0.0]
        for s in (0, 1):
            part = pl.ds(s * half, half)
            for k in (0, 1):
                there = here.at[2 * shard + k, part]
                pltpu.make_async_copy(there, there, sems.at[4 * shard + 2 * s + k]).wait()
            rows = rows_ref[:, s * half : (s + 1) * half]
            sums = [total + dot32(rows, here[2 * shard + k, part]) for k, total in enumerate(sums)]
        gate, up = sums
        columns = pl.ds(pl.multiple_of(shard * units, units), units)
        out_ref[:, columns] = (gate / (1.0 + jnp.exp(-gate)) * up).astype(jnp.bfloat16)
        return _

    lax.fori_loop(0, count, shard_of, 0)


def lead_kernel(near_ref, *refs, widths):
    pieces, (out_ref, stacked, sems) = refs[:-3], refs[-3:]
    units, at, pairs = pieces[0].shape[0], 0, []
    for i, width in enumerate(widths):
        for k in range(3):
            pairs.append((pieces[3 * i + k], stacked.at[pl.ds(k * units, units), pl.ds(at, width)]))
        at += width
    for copy in fetch(pairs, sems):
        copy.wait()

    for place in spans(at):
        out_ref[:, place] = dot32(near_ref[...], stacked[:, place])


def down_kernel(lead_ref, far_ref, *refs):
    pieces, (out_ref, far_weight, made, came, sent) = refs[:-5], refs[-5:]
    at, pairs = 0, []
    for piece in pieces:
        pairs.append((piece, far_weight.at[:, pl.ds(at, piece.shape[1])]))
        at += piece.shape[1]
    for copy in fetch(pairs, came):
        copy.wait()

    copies = []
    for i, place in enumerate(spans(at)):
        made[:, place] = (lead_ref[:, place] + dot32(far_ref[...], far_weight[:, place])).astype(jnp.bfloat16)
        copies.append(pltpu.make_async_copy(made.at[:, place], out_ref.at[:, place], sent.at[i]))
        copies[-1].start()
    for copy in copies:
        copy.wait()


def on_core(kernel, shape, operands, mib, scratch=(), out=pltpu.VMEM, away=0, kind=jnp.bfloat16):
    count = len(operands) - away
    return pl.pallas_call(
        kernel,
        out_shape=jax.ShapeDtypeStruct(shape, kind),
        in_specs=[pl.BlockSpec(memory_space=pltpu.VMEM)] * count + [pl.BlockSpec(memory_space=pltpu.HBM)] * away,
        out_specs=pl.BlockSpec(memory_space=out),
        scratch_shapes=list(scratch),
        compiler_params=pltpu.CompilerParams(vmem_limit_bytes=mib * MIB),
    )(*operands)


def mixer_kernel(place_ref, own_ref, left_ref, right_ref, first_ref, second_ref, weight_ref, out_ref):
    rows = own_ref.shape[0]
    weight = weight_ref[...]

    def put(ref, steps, offset):
        block = jnp.dot(ref[...], weight, preferred_element_type=jnp.float32).astype(jnp.bfloat16)
        at = ((place_ref[0] + steps) & 3) * rows + offset
        out_ref[pl.ds(pl.multiple_of(at, rows // 2), block.shape[0]), :] = block

    put(own_ref, 0, 0)
    put(left_ref, 3, 0)
    put(right_ref, 1, 0)
    put(first_ref, 2, 0)
    put(second_ref, 2, rows // 2)


def spans(width):
    return [pl.ds(at, min(COLUMNS, width - at)) for at in range(0, width, COLUMNS)]


def dot32(a, b):
    return jnp.dot(a, b, preferred_element_type=jnp.float32)


def local(
    out_gate,
    in_gate,
    conv_input,
    conv_taps,
    mixer_weight,
    expert_input,
    norm_gain,
    expert_gate,
    expert_up,
    expert_down,
    expert_ids,
    route_weight,
):
    row_count, model_width = in_gate.shape
    token_count = expert_input.shape[0]
    expert_count = lax.axis_size("ep")
    slot_cap = 4 * token_count // expert_count
    slots = expert_count * slot_cap
    vmem = pl.BlockSpec(memory_space=pltpu.VMEM)
    ids_t = expert_ids.T
    weight_t = route_weight.T

    gate, up, down = expert_gate[0], expert_up[0], expert_down[0]
    gates = from_sides(gate)
    ups = from_sides(up)
    gate_far = turn(gates[0], 1)
    up_far = turn(ups[1], -1)
    downs, at = [], 0
    for i, width in enumerate(PIECES):
        part = down[:, at : at + width]
        at += width
        sides = from_sides(part)
        far = turn(sides[i % 2], 1 - 2 * (i % 2))
        downs.append((part, *sides, far))

    outgoing = on_core(
        lambda *refs: dispatch_kernel(*refs, expert_count=expert_count, slot_cap=slot_cap),
        (slots, model_width),
        (ids_t, expert_input, norm_gain[None]),
        12,
    )
    arrived = lax.all_to_all(
        outgoing.reshape(expert_count, slot_cap, model_width), "ep", 0, 0, tiled=True
    ).reshape(slots, model_width)
    mix = on_core(
        lambda *refs: mix_kernel(*refs, expert_count=expert_count, slot_cap=slot_cap),
        (2 * token_count, slots),
        (ids_t, weight_t),
        8,
    )

    tap_span = CONV - 1
    product = in_gate.astype(jnp.float32) * conv_input.astype(jnp.float32)
    devices = expert_count * lax.axis_size("tp")
    earlier = lax.ppermute(
        product[row_count - tap_span :], ("ep", "tp"), [(i, i + 1) for i in range(devices - 1)]
    )
    padded = jnp.concatenate([earlier, product], axis=0)
    taps = conv_taps.astype(jnp.float32)
    smoothed = sum(padded[j : j + row_count] * taps[j] for j in range(CONV))
    gated = (out_gate.astype(jnp.float32) * smoothed).astype(jnp.bfloat16)

    units = gate.shape[1]

    def hidden(shards):
        weights = [w for shard in shards for w in shard]
        scratch = (
            pltpu.VMEM((len(weights), model_width, units), jnp.bfloat16),
            pltpu.SemaphoreType.DMA((2 * len(weights),)),
        )
        return on_core(
            lambda *refs: hidden_kernel(*refs, count=len(shards)),
            (slots, len(shards) * units),
            (arrived, *weights),
            4 * len(shards) + 6,
            scratch,
            away=len(weights),
        )

    near = hidden(((gate, up), (gates[0], ups[0]), (gates[1], ups[1])))
    far = hidden(((gate_far, up_far),))

    returned = []
    for chunk in CHUNKS:
        widths = [PIECES[piece] for piece in chunk]
        width = sum(widths)
        sides = [d for piece in chunk for d in downs[piece][:3]]
        lead = on_core(
            lambda *refs, widths=widths: lead_kernel(*refs, widths=widths),
            (slots, width),
            (near, *sides),
            12,
            (pltpu.VMEM((3 * units, width), jnp.bfloat16), pltpu.SemaphoreType.DMA((len(sides),))),
            away=len(sides),
            kind=jnp.float32,
        )
        scratch = (
            pltpu.VMEM((units, width), jnp.bfloat16),
            pltpu.VMEM((slots, width), jnp.bfloat16),
            pltpu.SemaphoreType.DMA((len(chunk),)),
            pltpu.SemaphoreType.DMA((len(spans(width)),)),
        )
        operands = (lead, far, *[downs[piece][3] for piece in chunk])
        result = on_core(down_kernel, (slots, width), operands, DOWN_MIB, scratch, pltpu.HBM, away=len(chunk))
        back = lax.all_to_all(result.reshape(expert_count, slot_cap, width), "ep", 0, 0, tiled=True)
        returned.append(back.reshape(slots, width))

    gated_sides = from_sides(gated)
    gated_far = from_opposite(*gated_sides)
    mixer_out = pl.pallas_call(
        mixer_kernel,
        out_shape=jax.ShapeDtypeStruct((4 * row_count, mixer_weight.shape[1]), jnp.bfloat16),
        in_specs=[pl.BlockSpec(memory_space=pltpu.SMEM)] + [vmem] * 6,
        out_specs=vmem,
        compiler_params=pltpu.CompilerParams(vmem_limit_bytes=8 * MIB),
        name="mixer",
    )(lax.axis_index("tp").reshape(1), gated, *gated_sides, *gated_far, mixer_weight)

    scratch = (
        pltpu.VMEM((token_count, model_width), jnp.bfloat16),
        pltpu.SemaphoreType.DMA((model_width // COLUMNS + len(CHUNKS),)),
    )
    experts_out = on_core(combine_kernel, (token_count, model_width), (mix, *returned), 8, scratch, pltpu.HBM)
    return (mixer_out, experts_out)


def solution(mesh):
    return jax.shard_map(
        local,
        mesh=mesh,
        in_specs=(
            P(("ep", "tp"), None),
            P(("ep", "tp"), None),
            P(("ep", "tp"), None),
            P(),
            P(None, "tp"),
            P(("ep", "tp"), None),
            P(),
            P("ep", None, "tp"),
            P("ep", None, "tp"),
            P("ep", "tp", None),
            P(("ep", "tp"), None),
            P(("ep", "tp"), None),
        ),
        out_specs=(P("ep", "tp"), P(("ep", "tp"), None)),
        check_vma=False,
    )
```
